32 devices in a mesh: sp: 8 (over z, core), tp: 4 (over y, x).
Axes of the slice: x: 2, y: 2, z: 4, core: 2. Of those that a mesh axis runs over, the one named last changes fastest.
Arguments:
- stream: bfloat16 [1024, 2048], P('sp'), may hold values from -6 to 6
- query_small: bfloat16 [1024, 1024], P('sp', 'tp'), may hold values from -6 to 6
- key_small: bfloat16 [1024, 1024], P('sp', 'tp'), may hold values from -6 to 6
- value_small: bfloat16 [1024, 1024], P('sp', 'tp'), may hold values from -6 to 6
- query_large: bfloat16 [1024, 2048], P('sp', 'tp'), may hold values from -6 to 6
- key_large: bfloat16 [1024, 2048], P('sp', 'tp'), may hold values from -6 to 6
- value_large: bfloat16 [1024, 2048], P('sp', 'tp'), may hold values from -6 to 6
- key_bias: bfloat16 [1024, 2, 16], P('sp', None, 'tp'), may hold values from -16 to 1
- out_small: bfloat16 [1024, 2048], P('tp'), may hold values from -0.75 to 0.75
- out_large: bfloat16 [2048, 2048], P('tp'), may hold values from -0.75 to 0.75
- gain_one: float32 [2048], replicated, may hold values from 0.1 to 1.9
- shift_one: float32 [2048], replicated, may hold values from -1.5 to 1.5
- gain_two: float32 [2048], replicated, may hold values from 0.1 to 1.9
- shift_two: float32 [2048], replicated, may hold values from -1.5 to 1.5
- expert_pick: int32 [1024, 2], P('sp'), may hold values from 0 to 7, as said below
- route_weight: float32 [1024, 2], P('sp'), may hold values from 0.2 to 1
- w_gate: bfloat16 [8, 2048, 4096], P('sp', None, 'tp'), may hold values from -0.125 to 0.125
- w_up: bfloat16 [8, 2048, 4096], P('sp', None, 'tp'), may hold values from -0.125 to 0.125
- w_down: bfloat16 [8, 4096, 2048], P('sp', 'tp'), may hold values from -0.09375 to 0.09375
Outputs:
- result: bfloat16 [1024, 2048], P(('sp', 'tp'))
The draws below stay inside these ranges and needn't reach their ends.
Inputs may be any that keep to these rules, and one draw needn't show every extreme that they name: In each aligned block of 128 positions (the positions of one index of sp), no expert is named more than 64 times, and in every block some expert is named exactly 64 times. The two experts of a position differ and lie in one group: equal values of expert_pick // 2.
All inputs are finite; a program needn't handle non-finite values.
Results may differ from the reference program's by a relative error of at most 0.017.
Values may be sent and summed in bfloat16 or wider, within the bound.
A program may use at most 64 MiB of HBM per device.

```python
import jax
import jax.numpy as jnp
from jax import lax

D = 2048
HEADS_PER_GROUP = 16
HEAD_SMALL = 64
HEAD_LARGE = 128
FF_E = 4096
GROUPS = 4
TOK_DEV = 128
SEQUENCE_LENGTH = 1024
EXPERTS = 8
PER_GROUP = 2
CAP = 64
N_TP = 4


def draw_key_bias(key, part):
    key_matrix = jax.random.split(key, 7)
    head_shape = (2, HEADS_PER_GROUP)
    fast_share = 0.5
    slow_low = 1.0
    slow_high = 2.0
    fast_heads = jax.random.uniform(key_matrix[0], head_shape) < fast_share
    slow_rate = jax.random.uniform(key_matrix[1], head_shape, minval=slow_low, maxval=slow_high) / SEQUENCE_LENGTH
    fast_rate = 1.0 / jax.random.uniform(key_matrix[2], head_shape, minval=30.0, maxval=100.0)
    rate = jnp.where(fast_heads, fast_rate, slow_rate)
    block_factor = jnp.exp(jax.random.uniform(key_matrix[3], (SEQUENCE_LENGTH // TOK_DEV, 2, HEADS_PER_GROUP), minval=-0.7, maxval=0.7))
    block_factor = jnp.repeat(block_factor, TOK_DEV, axis=0)
    baseline_logit = jnp.log(rate[None] * block_factor) - 0.5
    spike_mask = jax.random.uniform(key_matrix[4], (SEQUENCE_LENGTH, 2, HEADS_PER_GROUP)) < 2.0 / SEQUENCE_LENGTH
    spike_level = jax.random.uniform(key_matrix[5], (SEQUENCE_LENGTH, 2, HEADS_PER_GROUP), minval=0.2, maxval=0.5)
    spike_logit = jnp.log(spike_level / (1.0 - spike_level))
    perturbation_term = 0.3 * jax.random.normal(key_matrix[6], (SEQUENCE_LENGTH, 2, HEADS_PER_GROUP))
    sampled_values = jnp.where(spike_mask, spike_logit, baseline_logit + perturbation_term)
    return sampled_values.astype(jnp.float32).astype(jnp.bfloat16)


def value_field(key, columns):
    key_matrix = jax.random.split(key, 2)
    sampled_values = jnp.clip(jax.random.normal(key_matrix[1], (SEQUENCE_LENGTH, columns)), -6.0, 6.0)
    return sampled_values.astype(jnp.float32).astype(jnp.bfloat16)


def draw_value_small(key, part):
    return value_field(jax.random.fold_in(key, 101), HEADS_PER_GROUP * HEAD_SMALL)


def draw_value_large(key, part):
    return value_field(jax.random.fold_in(key, 202), HEADS_PER_GROUP * HEAD_LARGE)


def group_cycle(sub_key):
    return jax.random.permutation(sub_key, PER_GROUP).astype(jnp.int32)


def pick_block(key):
    key_matrix = jax.random.split(key, 4)
    order = jnp.argsort(jax.random.permutation(key_matrix[0], TOK_DEV)).astype(jnp.int32)
    group_cap = PER_GROUP * CAP // 2
    group_order = jax.random.permutation(key_matrix[1], GROUPS).astype(jnp.int32)
    cut_pair = jax.random.randint(key_matrix[2], (2,), group_cap, TOK_DEV + 1).astype(jnp.int32)
    cut_low = jnp.min(cut_pair)
    cut_high = jnp.max(cut_pair)
    bucket = (order >= group_cap).astype(jnp.int32) + (order >= cut_low).astype(jnp.int32) + (order >= cut_high).astype(jnp.int32)
    offsets = jnp.stack([jnp.int32(0), jnp.int32(group_cap), cut_low, cut_high])
    in_group = order - offsets[bucket]
    group_id = group_order[bucket]
    cycles = jax.vmap(group_cycle)(jax.random.split(key_matrix[3], GROUPS))
    first_pick = cycles[group_id, 2 * in_group % PER_GROUP]
    second_pick = cycles[group_id, (2 * in_group + 1) % PER_GROUP]
    return jnp.stack([group_id * PER_GROUP + first_pick, group_id * PER_GROUP + second_pick], axis=-1).astype(jnp.int32)


def draw_expert_pick(key, part):
    return jax.vmap(pick_block)(jax.random.split(key, SEQUENCE_LENGTH // TOK_DEV)).reshape(SEQUENCE_LENGTH, 2)


def level_of(key, extent, cuts, smallest, high):
    factor_of, own = 1.0, jax.random.fold_in(key, 6)
    for position, parts in cuts:
        heights = jnp.exp(jax.random.uniform(jax.random.fold_in(own, position), (parts,), jnp.float32, smallest / len(cuts), high / len(cuts)))
        factor_of = factor_of * jnp.repeat(heights, extent[position] // parts).reshape([-1 if axis == position else 1 for axis in range(len(extent))])
    return factor_of


def bell_draw(own_key, dims, scale, bound, cuts=(), held_as=jnp.bfloat16):
    values = scale * jax.random.normal(own_key, dims, jnp.float32)
    if cuts:
        values = values * level_of(own_key, dims, cuts, -0.22, 0.18)
    return jnp.clip(values, -bound, bound).astype(held_as)


def setup_inputs(seed: int = 0) -> dict:
    key_list = jax.random.split(jax.random.key(seed), 20)
    stream = bell_draw(key_list[0], (SEQUENCE_LENGTH, D), 1.0, 6.0, ((0, 8),))
    query_small = bell_draw(key_list[1], (SEQUENCE_LENGTH, HEADS_PER_GROUP * HEAD_SMALL), 1.0, 6.0, ((0, 8), (1, 4)))
    key_small = bell_draw(key_list[2], (SEQUENCE_LENGTH, HEADS_PER_GROUP * HEAD_SMALL), 1.0, 6.0, ((0, 8), (1, 4)))
    value_small = draw_value_small(jax.random.fold_in(key_list[19], 71), 0)
    query_large = bell_draw(key_list[4], (SEQUENCE_LENGTH, HEADS_PER_GROUP * HEAD_LARGE), 1.0, 6.0, ((0, 8), (1, 4)))
    key_large = bell_draw(key_list[5], (SEQUENCE_LENGTH, HEADS_PER_GROUP * HEAD_LARGE), 1.0, 6.0, ((0, 8), (1, 4)))
    value_large = draw_value_large(jax.random.fold_in(key_list[19], 71), 0)
    key_bias = draw_key_bias(jax.random.fold_in(key_list[19], 71), 0)
    out_small = bell_draw(key_list[8], (HEADS_PER_GROUP * HEAD_SMALL, D), (HEADS_PER_GROUP * (HEAD_SMALL + HEAD_LARGE) // 48) ** -0.5, 0.75, ((0, 4),))
    out_large = bell_draw(key_list[9], (HEADS_PER_GROUP * HEAD_LARGE, D), (HEADS_PER_GROUP * (HEAD_SMALL + HEAD_LARGE) // 48) ** -0.5, 0.75, ((0, 4),))
    gain_one = jnp.clip(1.0 + 0.18 * jax.random.normal(key_list[10], (D,), jnp.float32), 0.1, 1.9)
    shift_one = bell_draw(key_list[11], (D,), 0.3, 1.5, (), jnp.float32)
    gain_two = jnp.clip(1.0 + 0.18 * jax.random.normal(key_list[12], (D,), jnp.float32), 0.1, 1.9)
    shift_two = bell_draw(key_list[13], (D,), 0.3, 1.5, (), jnp.float32)
    expert_pick = draw_expert_pick(jax.random.fold_in(key_list[19], 71), 0)
    route_weight = jnp.clip(0.2 + 0.8 * jax.random.uniform(key_list[15], (SEQUENCE_LENGTH, 2), jnp.float32) ** level_of(key_list[15], (SEQUENCE_LENGTH, 2), ((0, 8),), -0.2, 0.2), 0.2, 1.0)
    w_gate = bell_draw(key_list[16], (EXPERTS, D, FF_E), D ** -0.5, 0.125, ((0, 8), (2, 4)))
    w_up = bell_draw(key_list[17], (EXPERTS, D, FF_E), D ** -0.5, 0.125, ((0, 8), (2, 4)))
    w_down = bell_draw(key_list[18], (EXPERTS, FF_E, D), FF_E ** -0.5, 0.09375, ((0, 8), (1, 4)))
    return dict(stream=stream, query_small=query_small, key_small=key_small, value_small=value_small, query_large=query_large, key_large=key_large, value_large=value_large, key_bias=key_bias, out_small=out_small, out_large=out_large, gain_one=gain_one, shift_one=shift_one, gain_two=gain_two, shift_two=shift_two, expert_pick=expert_pick, route_weight=route_weight, w_gate=w_gate, w_up=w_up, w_down=w_down)


ALPHA_RES = 2.0 ** 0.25
NORM_EPS = 1e-05

def layer_norm(inputs, gain_vec, shift_vec):
    average = lax.optimization_barrier(jnp.mean(inputs, axis=-1, keepdims=True))
    centred = inputs - average
    variance = lax.optimization_barrier(jnp.mean(centred * centred, axis=-1, keepdims=True))
    return centred * lax.rsqrt(variance + NORM_EPS) * gain_vec + shift_vec

def stick_head(queries, key_rows, value_rows, log_bias):
    score_scale = queries.shape[1] ** (-0.5)
    outputs = []
    for block in range(SEQUENCE_LENGTH // TOK_DEV):
        first_row = block * TOK_DEV
        last_row = first_row + TOK_DEV
        scores = jnp.dot(queries[first_row:last_row], key_rows[:last_row].T, preferred_element_type=jnp.float32)
        scores = scores * score_scale + log_bias[:last_row].astype(jnp.float32)[None, :]
        query_pos = first_row + jnp.arange(TOK_DEV)
        key_pos = jnp.arange(last_row)
        causal = key_pos[None, :] < query_pos[:, None]
        log_stay = jnp.where(causal, jax.nn.log_sigmoid(-scores), 0.0)
        later_sum = lax.cumsum(log_stay, axis=1, reverse=True) - log_stay
        stick = jnp.where(causal, jnp.exp(jax.nn.log_sigmoid(scores) + later_sum), 0.0)
        outputs.append(jnp.dot(stick.astype(jnp.bfloat16), value_rows[:last_row], preferred_element_type=jnp.float32))
    return jnp.concatenate(outputs, 0).astype(jnp.bfloat16)

def stick_group(queries, key_rows, value_rows, log_bias):
    head_size = queries.shape[1] // HEADS_PER_GROUP

    def split_heads(array):
        return array.reshape(SEQUENCE_LENGTH, HEADS_PER_GROUP, head_size).transpose(1, 0, 2)

    def one_head(packed):
        return stick_head(packed[0], packed[1], packed[2], packed[3])
    outputs = lax.map(one_head, (split_heads(queries), split_heads(key_rows), split_heads(value_rows), log_bias.T))
    return outputs.transpose(1, 0, 2).reshape(SEQUENCE_LENGTH, HEADS_PER_GROUP * head_size)

def reference(stream, query_small, key_small, value_small, query_large, key_large, value_large, key_bias, out_small, out_large, gain_one, shift_one, gain_two, shift_two, expert_pick, route_weight, w_gate, w_up, w_down):
    att_small = stick_group(query_small, key_small, value_small, key_bias[:, 0, :])
    att_large = stick_group(query_large, key_large, value_large, key_bias[:, 1, :])
    run_heads = HEADS_PER_GROUP // N_TP
    small_cols = run_heads * HEAD_SMALL
    large_cols = run_heads * HEAD_LARGE
    mixer_out = jnp.zeros((SEQUENCE_LENGTH, D), jnp.float32)
    for shard_index in range(N_TP):
        term = jnp.dot(att_small[:, shard_index * small_cols:(shard_index + 1) * small_cols], out_small[shard_index * small_cols:(shard_index + 1) * small_cols], preferred_element_type=jnp.float32)
        term = term + jnp.dot(att_large[:, shard_index * large_cols:(shard_index + 1) * large_cols], out_large[shard_index * large_cols:(shard_index + 1) * large_cols], preferred_element_type=jnp.float32)
        mixer_out = mixer_out + lax.optimization_barrier(term.astype(jnp.bfloat16)).astype(jnp.float32)
    normed = layer_norm(ALPHA_RES * stream.astype(jnp.float32) + mixer_out, gain_one, shift_one).astype(jnp.bfloat16)
    blocks = SEQUENCE_LENGTH // TOK_DEV
    picks = expert_pick.reshape(blocks, TOK_DEV * 2)
    one_hot = (picks[:, :, None] == jnp.arange(EXPERTS)[None, None, :]).astype(jnp.int32)
    slot_rank = lax.optimization_barrier(jnp.sum((jnp.cumsum(one_hot, axis=1) - one_hot) * one_hot, axis=2)).astype(jnp.int32)
    block_ids = jnp.broadcast_to(jnp.arange(blocks, dtype=jnp.int32)[:, None], picks.shape)
    token_of = (jnp.arange(TOK_DEV * 2, dtype=jnp.int32) // 2)[None, :] + block_ids * TOK_DEV
    slot_table = jnp.zeros((EXPERTS, blocks, CAP), jnp.int32).at[picks, block_ids, slot_rank].set(token_of)
    width = FF_E // N_TP

    def expert_rows(packed):
        table, gate_w, up_w, down_w = packed
        rows_in = normed[table.reshape(-1)]
        gate = jnp.dot(rows_in, gate_w, preferred_element_type=jnp.float32)
        upper = jnp.dot(rows_in, up_w, preferred_element_type=jnp.float32)
        hidden = (jax.nn.silu(gate) * upper).astype(jnp.bfloat16)
        running = jnp.zeros((rows_in.shape[0], D), jnp.float32)
        for shard_index in range(N_TP):
            term = jnp.dot(hidden[:, shard_index * width:(shard_index + 1) * width], down_w[shard_index * width:(shard_index + 1) * width], preferred_element_type=jnp.float32)
            running = running + lax.optimization_barrier(term.astype(jnp.bfloat16)).astype(jnp.float32)
        return running.astype(jnp.bfloat16)
    results = lax.map(expert_rows, (slot_table, w_gate, w_up, w_down)).reshape(EXPERTS, blocks, CAP, D)
    chosen = results[picks, block_ids, slot_rank].reshape(SEQUENCE_LENGTH, 2, D).astype(jnp.float32)
    expert_mix = chosen[:, 0] * route_weight[:, 0:1] + chosen[:, 1] * route_weight[:, 1:2]
    return layer_norm(ALPHA_RES * normed.astype(jnp.float32) + expert_mix, gain_two, shift_two).astype(jnp.bfloat16)
```

```python
import functools

import jax
import jax.numpy as jnp
from jax import lax
from jax.experimental import pallas as pl
from jax.experimental.pallas import tpu as pltpu
from jax.sharding import PartitionSpec as P

HEAD_SMALL = 64
HEAD_LARGE = 128


ALPHA_RES = 2.0**0.25
NORM_EPS = 1e-05


def layer_norm(inputs, gain_vec, shift_vec):
    average = jnp.mean(inputs, axis=-1, keepdims=True)
    centred = inputs - average
    variance = jnp.mean(centred * centred, axis=-1, keepdims=True)
    return centred * lax.rsqrt(variance + NORM_EPS) * gain_vec + shift_vec


def stick_group(queries, key_rows, value_rows, log_bias, position):
    query_count = queries.shape[0]
    head_count = queries.shape[1]
    value_size = value_rows.shape[2]
    key_span = 4 * query_count
    score_scale = queries.shape[2] ** (-0.5)
    query_pos = position * query_count + jnp.arange(query_count, dtype=jnp.int32)
    block_count = (position * query_count + query_count + key_span - 1) // key_span

    def visit_block(turn_index, carry):
        running, stay_sum = carry
        first_key = (block_count - 1 - turn_index) * key_span
        key_block = lax.dynamic_slice_in_dim(key_rows, first_key, key_span, 0)
        value_block = lax.dynamic_slice_in_dim(value_rows, first_key, key_span, 0)
        bias_block = lax.dynamic_slice_in_dim(log_bias, first_key, key_span, 0).astype(jnp.float32)
        scores = jnp.einsum("qhd,khd->hqk", queries, key_block, preferred_element_type=jnp.float32)
        scores = scores * score_scale + bias_block.T[:, None, :]
        key_pos = first_key + jnp.arange(key_span, dtype=jnp.int32)
        causal = (key_pos[None, :] < query_pos[:, None])[None]
        log_stay = jnp.where(causal, jax.nn.log_sigmoid(-scores), 0.0)
        later_sum = lax.cumsum(log_stay, axis=2, reverse=True) - log_stay + stay_sum[:, :, None]
        stick_weight = jnp.where(
            causal, jnp.exp(jax.nn.log_sigmoid(scores) + later_sum), 0.0
        ).astype(jnp.bfloat16)
        running = running + jnp.einsum(
            "hqk,khd->qhd", stick_weight, value_block, preferred_element_type=jnp.float32
        )
        stay_sum = stay_sum + jnp.sum(log_stay, axis=2)
        return (running, stay_sum)

    start_total = jnp.zeros((query_count, head_count, value_size), jnp.float32)
    start_stay = jnp.zeros((head_count, query_count), jnp.float32)
    running, stay_sum = lax.fori_loop(0, block_count, visit_block, (start_total, start_stay))
    return running.reshape(query_count, head_count * value_size).astype(jnp.bfloat16)


def split_heads(array, head_size):
    return array.reshape(array.shape[0], array.shape[1] // head_size, head_size)


def local(
    stream,
    query_small,
    key_small,
    value_small,
    query_large,
    key_large,
    value_large,
    key_bias,
    out_small,
    out_large,
    gain_one,
    shift_one,
    gain_two,
    shift_two,
    expert_pick,
    route_weight,
    w_gate,
    w_up,
    w_down,
):
    row_count = stream.shape[0]
    position = lax.axis_index("sp")
    gathered = (
        lax.all_gather(key_small, "sp", axis=0, tiled=True),
        lax.all_gather(value_small, "sp", axis=0, tiled=True),
        lax.all_gather(key_large, "sp", axis=0, tiled=True),
        lax.all_gather(value_large, "sp", axis=0, tiled=True),
        lax.all_gather(key_bias, "sp", axis=0, tiled=True),
    )
    att_small = stick_group(
        split_heads(query_small, HEAD_SMALL),
        split_heads(gathered[0], HEAD_SMALL),
        split_heads(gathered[1], HEAD_SMALL),
        gathered[4][:, 0],
        position,
    )
    att_large = stick_group(
        split_heads(query_large, HEAD_LARGE),
        split_heads(gathered[2], HEAD_LARGE),
        split_heads(gathered[3], HEAD_LARGE),
        gathered[4][:, 1],
        position,
    )
    partial_value = jnp.dot(att_small, out_small, preferred_element_type=jnp.float32)
    partial_value = partial_value + jnp.dot(
        att_large, out_large, preferred_element_type=jnp.float32
    )
    mixer_out = lax.psum(partial_value.astype(jnp.bfloat16), "tp").astype(jnp.float32)
    normed = layer_norm(
        ALPHA_RES * stream.astype(jnp.float32) + mixer_out, gain_one, shift_one
    ).astype(jnp.bfloat16)
    experts = w_gate.shape[0] * lax.axis_size("sp")
    capacity = 4 * row_count // experts
    tp_count = lax.axis_size("tp")
    tp_index = lax.axis_index("tp")
    per_lane = capacity // tp_count
    flat_picks = expert_pick.reshape(-1)
    one_hot = (flat_picks[:, None] == jnp.arange(experts, dtype=jnp.int32)[None, :]).astype(
        jnp.int32
    )
    slot_rank = jnp.sum((jnp.cumsum(one_hot, axis=0) - one_hot) * one_hot, axis=1)
    slot_index = (flat_picks * capacity + slot_rank).reshape(row_count, 2)

    def selector(first_slot, slot_count):
        target = (
            jnp.arange(experts, dtype=jnp.int32)[:, None] * capacity
            + first_slot
            + jnp.arange(slot_count, dtype=jnp.int32)[None, :]
        ).reshape(-1)
        return [target[:, None] == slot_index[None, :, pick_index] for pick_index in range(2)]

    own_select = selector(tp_index * per_lane, per_lane)
    all_select = selector(0, capacity)
    placing = (all_select[0] | all_select[1]).astype(jnp.bfloat16)
    outgoing = jnp.dot(placing, normed, preferred_element_type=jnp.float32).astype(jnp.bfloat16)
    arrived = lax.all_to_all(
        outgoing.reshape(experts, capacity, normed.shape[1]),
        "sp",
        split_axis=0,
        concat_axis=0,
        tiled=True,
    )
    flat_rows = arrived.reshape(-1, arrived.shape[2])
    gate = jnp.dot(flat_rows, w_gate[0], preferred_element_type=jnp.float32)
    upper = jnp.dot(flat_rows, w_up[0], preferred_element_type=jnp.float32)
    hidden = (jax.nn.silu(gate) * upper).astype(jnp.bfloat16)
    expert_terms = jnp.dot(hidden, w_down[0], preferred_element_type=jnp.float32).reshape(
        arrived.shape
    )
    summed = lax.psum_scatter(
        expert_terms.astype(jnp.bfloat16), "tp", scatter_dimension=1, tiled=True
    )
    returned = lax.all_to_all(summed, "sp", split_axis=0, concat_axis=0, tiled=True).reshape(
        experts * per_lane, normed.shape[1]
    )
    picked_first = jnp.einsum(
        "sr,sd->rd",
        own_select[0].astype(jnp.bfloat16),
        returned,
        preferred_element_type=jnp.float32,
    )
    picked_second = jnp.einsum(
        "sr,sd->rd",
        own_select[1].astype(jnp.bfloat16),
        returned,
        preferred_element_type=jnp.float32,
    )
    partial_mix = route_weight[:, 0:1] * picked_first + route_weight[:, 1:2] * picked_second
    expert_mix = lax.psum_scatter(
        partial_mix.astype(jnp.bfloat16), "tp", scatter_dimension=0, tiled=True
    ).astype(jnp.float32)
    own_count = row_count // tp_count
    own_rows = lax.dynamic_slice_in_dim(normed, tp_index * own_count, own_count, 0).astype(
        jnp.float32
    )
    return layer_norm(ALPHA_RES * own_rows + expert_mix, gain_two, shift_two).astype(jnp.bfloat16)


GROUPS = 4


def fast_kernel(
    dims,
    qs_ref, ks_ref, vs_ref, ql_ref, kl_ref, vl_ref, bias_ref, stream_ref, os_ref, ol_ref,
    g1_ref, b1_ref, g2_ref, b2_ref, pick_ref, route_ref, wg_ref, wu_ref, wd_ref,
    out_ref,
    pack_a, pack_v, rq, rk, rv, rb, aq, ak, ao, ra, wos, wol, strm, pb, rp, st, rst, normed,
    place, xs, wsend, wrecv, ag, wg, wu, wd, hid, own_y, cs, cr, ts, rr, zs, zr, fs, fr,
    load_sem, q_send, q_recv, a_send, a_recv, p_send, p_recv, s_send, s_recv,
    x_send, x_recv, w_send, w_recv, g_send, g_recv, h_send, h_recv, c_send, c_recv,
    t_send, t_recv, z_send, z_recv, f_send, f_recv,
):
    n_sp, n_tp, rows, cols, cap, small_heads, hs, hl = dims
    f32, bf16 = jnp.float32, jnp.bfloat16
    sp = lax.axis_index("sp")
    tp = lax.axis_index("tp")
    core = lax.rem(sp, 2)
    chip = lax.div(sp, 2)
    sibling = sp + 1 - 2 * core
    n_z = n_sp // 2
    is_small = sp < small_heads
    large_heads = n_sp - small_heads
    ffw = wg_ref.shape[2]
    width = n_tp * cols

    def mesh_copy(src, dst, send, recv, target):
        return pltpu.make_async_remote_copy(
            src_ref=src, dst_ref=dst, send_sem=send, recv_sem=recv,
            device_id=target, device_id_type=pl.DeviceIdType.MESH,
        )

    def sp_at(j):
        return (j, tp)

    def tp_at(j):
        return (sp, j)

    barrier = pltpu.get_barrier_semaphore()
    for k in range(1, n_sp):
        pl.semaphore_signal(barrier, inc=1, device_id=sp_at(lax.rem(sp + k, n_sp)), device_id_type=pl.DeviceIdType.MESH)
    for k in range(1, n_tp):
        pl.semaphore_signal(barrier, inc=1, device_id=tp_at(lax.rem(tp + k, n_tp)), device_id_type=pl.DeviceIdType.MESH)

    own_cols = pl.ds(pl.multiple_of(tp * cols, cols), cols)
    loads = [
        pltpu.make_async_copy(os_ref, wos, load_sem.at[0]),
        pltpu.make_async_copy(ol_ref, wol, load_sem.at[1]),
        pltpu.make_async_copy(stream_ref.at[:, own_cols], strm, load_sem.at[2]),
        pltpu.make_async_copy(wg_ref.at[0], wg, load_sem.at[3]),
        pltpu.make_async_copy(wu_ref.at[0], wu, load_sem.at[4]),
        pltpu.make_async_copy(wd_ref.at[0], wd, load_sem.at[5]),
    ]
    for load in loads:
        load.start()

    for h in range(small_heads):
        part = slice(h * hs, (h + 1) * hs)
        pack_a[h] = jnp.concatenate([qs_ref[:, part], ks_ref[:, part]], axis=1)
        pack_v[h] = jnp.concatenate([vs_ref[:, part], jnp.zeros((rows, hl - hs), bf16)], axis=1)

    pl.semaphore_wait(barrier, n_sp + n_tp - 2)

    def head_copies(j, slot):
        if j < small_heads:
            pairs = [(0, pack_a.at[j], rq), (2, pack_v.at[j], rv)]
        else:
            part = pl.ds((j - small_heads) * hl, hl)
            pairs = [(0, ql_ref.at[:, part], rq), (1, kl_ref.at[:, part], rk), (2, vl_ref.at[:, part], rv)]
        pairs.append((3, bias_ref.at[j], rb))
        return [(kind, src, dst.at[slot]) for kind, src, dst in pairs]

    for j in range(n_sp):
        @pl.when(j != sp)
        def _():
            for kind, src, dst in head_copies(j, sp):
                mesh_copy(src, dst, q_send.at[kind, j], q_recv.at[kind, sp], sp_at(j)).start()

        @pl.when(j == sp)
        def _():
            for kind, src, dst in head_copies(j, j):
                pltpu.make_async_copy(src, dst, q_recv.at[kind, j]).start()

    group = lax.div(pick_ref[0:1, :], 2)
    first_even = lax.rem(pick_ref[0:1, :], 2) == 0
    sub8 = lax.broadcasted_iota(jnp.int32, (8, rows), 0)
    one_hot = (sub8 == group).astype(f32)
    sub_r = lax.broadcasted_iota(jnp.int32, (rows, rows), 0)
    lane_r = lax.broadcasted_iota(jnp.int32, (rows, rows), 1)
    before = (sub_r < lane_r).astype(f32).astype(bf16)
    counts = jnp.dot(one_hot.astype(bf16), before, preferred_element_type=f32)
    rank = jnp.sum(one_hot * counts, axis=0, keepdims=True).astype(jnp.int32)
    slot_row = group * cap + rank
    slot_iota = lax.broadcasted_iota(jnp.int32, (GROUPS * cap, rows), 0)
    place[...] = (slot_iota == slot_row).astype(f32).astype(bf16)
    w_even = jnp.where(first_even, route_ref[0:1, :], route_ref[1:2, :])
    w_odd = jnp.where(first_even, route_ref[1:2, :], route_ref[0:1, :])
    w8 = jnp.where(sub8 == 0, w_even, jnp.where(sub8 == 1, w_odd, 0.0))
    w_hi = w8.astype(bf16)
    w_lo = (w8 - w_hi.astype(f32)).astype(bf16)
    for g in range(GROUPS):
        pick_g = ((sub_r == slot_row - g * cap) & (sub_r < cap)).astype(f32).astype(bf16)
        last = (((1,), (1,)), ((), ()))
        wsend[g] = lax.dot_general(w_hi, pick_g, last, preferred_element_type=f32) + lax.dot_general(
            w_lo, pick_g, last, preferred_element_type=f32
        )

    for j in range(n_sp):
        for kind in (0, 2, 3):
            dst = (rq, None, rv, rb)[kind].at[j]
            pltpu.make_async_copy(dst, dst, q_recv.at[kind, j]).wait()

    @pl.when(jnp.logical_not(is_small))
    def _():
        for j in range(n_sp):
            pltpu.make_async_copy(rk.at[j], rk.at[j], q_recv.at[1, j]).wait()
            aq[pl.ds(j * rows, rows), :] = rq[j]
            ak[pl.ds(j * rows, rows), :] = rk[j]

    @pl.when(is_small)
    def _():
        lane = lax.broadcasted_iota(jnp.int32, (rows, hl), 1)
        for j in range(n_sp):
            both = rq[j]
            aq[pl.ds(j * rows, rows), :] = jnp.where(lane < hs, both, jnp.zeros_like(both))
            ak[pl.ds(j * rows, rows), :] = jnp.concatenate([both[:, hs:], both[:, :hs]], axis=1)

    for j in range(n_sp):
        @pl.when(j != sp)
        def _():
            for kind, src, dst in head_copies(j, sp):
                mesh_copy(src, dst, q_send.at[kind, j], q_recv.at[kind, sp], sp_at(j)).wait_send()

    scale = jnp.where(is_small, hs**-0.5, hl**-0.5).astype(f32)
    span = 2 * rows
    sub_t = lax.broadcasted_iota(jnp.int32, (span, span), 0)
    lane_t = lax.broadcasted_iota(jnp.int32, (span, span), 1)
    tri = (sub_t >= lane_t).astype(f32).astype(bf16)
    causal = lane_t < sub_t

    def tile(query, kj, diagonal, total, later):
        keys = ak[pl.ds(pl.multiple_of(kj * span, span), span), :]
        log_odds = jnp.concatenate([rb[2 * kj, 0:1, :], rb[2 * kj + 1, 0:1, :]], axis=1)
        score = lax.dot_general(query, keys, (((1,), (1,)), ((), ())), preferred_element_type=f32)
        score = score * scale + log_odds
        soft = jnp.maximum(score, 0.0) + jnp.log(1.0 + jnp.exp(-jnp.abs(score)))
        if diagonal:
            soft = jnp.where(causal, soft, 0.0)
        high = soft.astype(bf16)
        low = (soft - high.astype(f32)).astype(bf16)
        run = jnp.dot(high, tri, preferred_element_type=f32) + jnp.dot(low, tri, preferred_element_type=f32)
        stick = jnp.exp(score - run - later)
        if diagonal:
            stick = jnp.where(causal, stick, 0.0)
        values = jnp.concatenate([rv[2 * kj], rv[2 * kj + 1]], axis=0)
        total = total + jnp.dot(stick.astype(bf16), values, preferred_element_type=f32)
        return total, later + run[:, 0:1]

    for qi in range(n_sp // 2):
        query = aq[qi * span:(qi + 1) * span, :]
        carry = tile(query, qi, True, jnp.zeros((span, hl), f32), jnp.zeros((span, 1), f32))
        if qi:
            def visit(turn, carry):
                return tile(query, qi - 1 - turn, False, *carry)
            carry = lax.fori_loop(0, qi, visit, carry)
        for half in range(2):
            d = 2 * qi + half
            ao[d] = carry[0][half * rows:(half + 1) * rows].astype(bf16)
        for half in range(2):
            d = 2 * qi + half

            @pl.when(d != sp)
            def _():
                mesh_copy(ao.at[d], ra.at[sp], a_send.at[d], a_recv.at[sp], sp_at(d)).start()

            @pl.when(d == sp)
            def _():
                pltpu.make_async_copy(ao.at[d], ra.at[d], a_recv.at[d]).start()

    for load in loads[:3]:
        load.wait()
    for j in range(n_sp):
        pltpu.make_async_copy(ra.at[j], ra.at[j], a_recv.at[j]).wait()
    att_small = jnp.concatenate([ra[j][:, :hs] for j in range(small_heads)], axis=1)
    att_large = jnp.concatenate([ra[j] for j in range(small_heads, n_sp)], axis=1)

    def tp_wait_recv(buf, sem, src):
        pltpu.make_async_copy(buf.at[src], buf.at[src], sem.at[src]).wait()

    for k in range(1, n_tp + 1):
        t = lax.rem(tp + k, n_tp)
        part = pl.ds(pl.multiple_of(t * cols, cols), cols)
        term = jnp.dot(att_small, wos[:, part], preferred_element_type=f32)
        term = term + jnp.dot(att_large, wol[:, part], preferred_element_type=f32)
        pb[k - 1] = term.astype(bf16)
        if k < n_tp:
            mesh_copy(pb.at[k - 1], rp.at[tp], p_send.at[k], p_recv.at[tp], tp_at(t)).start()
    mixed = ALPHA_RES * strm[...].astype(f32) + pb[n_tp - 1].astype(f32)
    for k in range(1, n_tp):
        src = lax.rem(tp + k, n_tp)
        tp_wait_recv(rp, p_recv, src)
        mixed = mixed + rp[src].astype(f32)

    eye = sub_r == lane_r

    def to_row(column):
        return jnp.sum(jnp.where(eye, column, 0.0), axis=0, keepdims=True)

    def to_column(row):
        return jnp.sum(jnp.where(eye, row, 0.0), axis=1, keepdims=True)

    own_mean = jnp.mean(mixed, axis=1, keepdims=True)
    centred = mixed - own_mean
    own_square = jnp.sum(centred * centred, axis=1, keepdims=True)
    mean_row, square_row = to_row(own_mean), to_row(own_square)
    st[...] = jnp.where(sub8 == 0, mean_row, square_row)
    for k in range(1, n_tp):
        t = lax.rem(tp + k, n_tp)
        mesh_copy(st, rst.at[tp], s_send.at[k], s_recv.at[tp], tp_at(t)).start()
    means, squares = [mean_row], [square_row]
    for k in range(1, n_tp):
        src = lax.rem(tp + k, n_tp)
        tp_wait_recv(rst, s_recv, src)
        means.append(rst[src, 0:1, :])
        squares.append(rst[src, 1:2, :])
    full_mean = sum(means) / n_tp
    spread = sum(squares) + cols * sum((m - full_mean) * (m - full_mean) for m in means)
    scale_row = lax.rsqrt(spread / width + NORM_EPS)
    norm_val = (mixed - to_column(full_mean)) * to_column(scale_row) * g1_ref[:, own_cols] + b1_ref[:, own_cols]
    normed[...] = norm_val.astype(bf16)

    for g in range(GROUPS):
        xs[g] = jnp.dot(place[g * cap:(g + 1) * cap, :], normed[...], preferred_element_type=f32).astype(bf16)
    for k in range(n_z):
        g = lax.rem(chip + k, n_z)
        dst = ag.at[core, tp, chip]
        if k == 0:
            pltpu.make_async_copy(xs.at[g], dst, x_recv.at[chip]).start()
        else:
            mesh_copy(xs.at[g], dst, x_send.at[k], x_recv.at[chip], sp_at(2 * g + core)).start()
    for k in range(n_sp):
        j = lax.rem(sp + k, n_sp)
        if k == 0:
            pltpu.make_async_copy(wsend.at[chip], wrecv.at[sp], w_recv.at[sp]).start()
        else:
            mesh_copy(wsend.at[lax.div(j, 2)], wrecv.at[sp], w_send.at[k], w_recv.at[sp], sp_at(j)).start()

    for k in range(n_z):
        z = lax.rem(chip + k, n_z)
        piece = ag.at[core, tp, z]
        pltpu.make_async_copy(piece, piece, x_recv.at[z]).wait()
        for m in range(1, n_tp):
            t = lax.rem(tp + m, n_tp)
            mesh_copy(piece, piece, g_send.at[m, z], g_recv.at[tp, z], tp_at(t)).start()
        mesh_copy(piece, piece, h_send.at[tp, z], h_recv.at[tp, z], sp_at(sibling)).start()
    for load in loads[3:]:
        load.wait()
    for k in range(n_z):
        z = lax.rem(chip + k, n_z)
        for m in range(1, n_tp):
            t = lax.rem(tp + m, n_tp)
            piece = ag.at[core, t, z]
            pltpu.make_async_copy(piece, piece, g_recv.at[t, z]).wait()
            mesh_copy(piece, piece, h_send.at[t, z], h_recv.at[t, z], sp_at(sibling)).start()

    half_rows = n_z * cap
    lane_c = lax.broadcasted_iota(jnp.int32, (cap, rows), 1)
    sub_c = lax.broadcasted_iota(jnp.int32, (cap, rows), 0)
    for j in range(n_sp):
        pltpu.make_async_copy(wrecv.at[j], wrecv.at[j], w_recv.at[j]).wait()

    def slot_weights(c):
        parts = []
        for z in range(n_z):
            row = wrecv[2 * z + c, pl.ds(core, 1), :]
            parts.append(jnp.sum(jnp.where(sub_c == lane_c, row, 0.0), axis=1, keepdims=True))
        return jnp.concatenate(parts, axis=0)

    def up_proj(c):
        step = min(256, ffw)

        def body(n, carry):
            part = pl.ds(pl.multiple_of(n * step, step), step)
            gate = jnp.zeros((half_rows, step), f32)
            upper = jnp.zeros((half_rows, step), f32)
            for t in range(n_tp):
                x = ag[c, t].reshape(half_rows, cols)
                gate = gate + jnp.dot(x, wg[t * cols:(t + 1) * cols, part], preferred_element_type=f32)
                upper = upper + jnp.dot(x, wu[t * cols:(t + 1) * cols, part], preferred_element_type=f32)
            hid[:, part] = (gate / (1.0 + jnp.exp(-gate)) * upper).astype(bf16)
            return carry

        lax.fori_loop(0, ffw // step, body, 0)

    def down_proj(t, weights):
        part = pl.ds(pl.multiple_of(t * cols, cols), cols)
        return jnp.dot(hid[...], wd[:, part], preferred_element_type=f32) * weights

    other = 1 - core
    up_proj(core)
    own_weights = slot_weights(core)
    for k in range(1, n_tp + 1):
        t = lax.rem(tp + k, n_tp)
        own_y[k - 1] = down_proj(t, own_weights)
    for t in range(n_tp):
        for z in range(n_z):
            piece = ag.at[other, t, z]
            pltpu.make_async_copy(piece, piece, h_recv.at[t, z]).wait()
    up_proj(other)
    other_weights = slot_weights(other)
    for k in range(1, n_tp + 1):
        t = lax.rem(tp + k, n_tp)
        cs[k - 1] = down_proj(t, other_weights).astype(bf16)
        mesh_copy(cs.at[k - 1], cr.at[k - 1], c_send.at[k - 1], c_recv.at[k - 1], sp_at(sibling)).start()
    summed = None
    for k in range(1, n_tp + 1):
        t = lax.rem(tp + k, n_tp)
        pltpu.make_async_copy(cr.at[k - 1], cr.at[k - 1], c_recv.at[k - 1]).wait()
        both = own_y[k - 1] + cr[k - 1].astype(f32)
        if k < n_tp:
            ts[k - 1] = both.astype(bf16)
            mesh_copy(ts.at[k - 1], rr.at[tp], t_send.at[k], t_recv.at[tp], tp_at(t)).start()
        else:
            own_y[k - 1] = both
    for k in range(1, n_tp):
        tp_wait_recv(rr, t_recv, lax.rem(tp + k, n_tp))
    for k in range(1, n_z + 1):
        z = lax.rem(chip + k, n_z)
        part = pl.ds(pl.multiple_of(z * cap, cap), cap)
        total = own_y[n_tp - 1, part, :]
        for m in range(1, n_tp):
            total = total + rr[lax.rem(tp + m, n_tp), part, :].astype(f32)
        zs[k - 1] = total.astype(bf16)
        if k < n_z:
            mesh_copy(zs.at[k - 1], zr.at[chip], z_send.at[k], z_recv.at[chip], sp_at(2 * z + core)).start()
        else:
            pltpu.make_async_copy(zs.at[k - 1], zr.at[chip], z_recv.at[chip]).start()
    for z in range(n_z):
        pltpu.make_async_copy(zr.at[z], zr.at[z], z_recv.at[z]).wait()
    expert_mix = lax.dot_general(
        place[...], zr[...].reshape(n_z * cap, cols), (((0,), (0,)), ((), ())), preferred_element_type=f32
    )
    final = ALPHA_RES * normed[...].astype(f32) + expert_mix
    own_rows = rows // n_tp
    for t in range(n_tp):
        fs[t] = final[t * own_rows:(t + 1) * own_rows]
    for k in range(1, n_tp):
        t = lax.rem(tp + k, n_tp)
        mesh_copy(fs.at[t], fr.at[tp], f_send.at[k], f_recv.at[tp], tp_at(t)).start()
    keep = pltpu.make_async_copy(fs.at[tp], fr.at[tp], f_recv.at[tp])
    keep.start()
    for t in range(n_tp):
        tp_wait_recv(fr, f_recv, t)
    blocks = [fr[t] for t in range(n_tp)]
    average = sum(jnp.sum(b, axis=1, keepdims=True) for b in blocks) / width
    blocks = [b - average for b in blocks]
    variance = sum(jnp.sum(b * b, axis=1, keepdims=True) for b in blocks) / width
    inverse = lax.rsqrt(variance + NORM_EPS)
    for t in range(n_tp):
        part = slice(t * cols, (t + 1) * cols)
        out_ref[:, part] = (blocks[t] * inverse * g2_ref[:, part] + b2_ref[:, part]).astype(bf16)

    for d in range(n_sp):
        @pl.when(d != sp)
        def _():
            mesh_copy(ao.at[d], ra.at[sp], a_send.at[d], a_recv.at[sp], sp_at(d)).wait_send()
    for k in range(1, n_sp):
        j = lax.rem(sp + k, n_sp)
        mesh_copy(wsend.at[lax.div(j, 2)], wrecv.at[sp], w_send.at[k], w_recv.at[sp], sp_at(j)).wait_send()
    for k in range(1, n_tp):
        t = lax.rem(tp + k, n_tp)
        mesh_copy(pb.at[k - 1], rp.at[tp], p_send.at[k], p_recv.at[tp], tp_at(t)).wait_send()
        mesh_copy(st, rst.at[tp], s_send.at[k], s_recv.at[tp], tp_at(t)).wait_send()
        mesh_copy(ts.at[k - 1], rr.at[tp], t_send.at[k], t_recv.at[tp], tp_at(t)).wait_send()
        mesh_copy(fs.at[t], fr.at[tp], f_send.at[k], f_recv.at[tp], tp_at(t)).wait_send()
        for z in range(n_z):
            piece = ag.at[core, tp, z]
            mesh_copy(piece, piece, g_send.at[k, z], g_recv.at[tp, z], tp_at(t)).wait_send()
    for k in range(1, n_z):
        g = lax.rem(chip + k, n_z)
        mesh_copy(xs.at[g], ag.at[core, tp, chip], x_send.at[k], x_recv.at[chip], sp_at(2 * g + core)).wait_send()
        mesh_copy(zs.at[k - 1], zr.at[chip], z_send.at[k], z_recv.at[chip], sp_at(2 * g + core)).wait_send()
    for t in range(n_tp):
        mesh_copy(cs.at[t], cr.at[t], c_send.at[t], c_recv.at[t], sp_at(sibling)).wait_send()
        for z in range(n_z):
            piece = ag.at[core, t, z]
            mesh_copy(piece, piece, h_send.at[t, z], h_recv.at[t, z], sp_at(sibling)).wait_send()


def fast_local(
    stream, query_small, key_small, value_small, query_large, key_large, value_large, key_bias,
    out_small, out_large, gain_one, shift_one, gain_two, shift_two, expert_pick, route_weight,
    w_gate, w_up, w_down,
):
    f32, bf16 = jnp.float32, jnp.bfloat16
    n_sp, n_tp = lax.axis_size("sp"), lax.axis_size("tp")
    rows, width = stream.shape
    cols = width // n_tp
    hs, hl = HEAD_SMALL, HEAD_LARGE
    small_heads = query_small.shape[1] // hs
    cap = 4 * rows // (w_gate.shape[0] * n_sp)
    n_z = n_sp // 2
    ffw = w_gate.shape[2]
    bias = key_bias.astype(f32).transpose(1, 2, 0).reshape(n_sp, 1, rows)
    bias = jnp.broadcast_to(bias, (n_sp, 8, rows))
    vmem = pl.BlockSpec(memory_space=pltpu.VMEM)
    hbm = pl.BlockSpec(memory_space=pl.ANY)
    dma = pltpu.SemaphoreType.DMA
    V = pltpu.VMEM
    half = n_z * cap
    scratch = [
        V((small_heads, rows, hl), bf16), V((small_heads, rows, hl), bf16),
        V((n_sp, rows, hl), bf16), V((n_sp, rows, hl), bf16), V((n_sp, rows, hl), bf16),
        V((n_sp, 8, rows), f32),
        V((n_sp * rows, hl), bf16), V((n_sp * rows, hl), bf16),
        V((n_sp, rows, hl), bf16), V((n_sp, rows, hl), bf16),
        V(out_small.shape, bf16), V(out_large.shape, bf16), V((rows, cols), bf16),
        V((n_tp, rows, cols), bf16), V((n_tp, rows, cols), bf16),
        V((8, rows), f32), V((n_tp, 8, rows), f32), V((rows, cols), bf16),
        V((GROUPS * cap, rows), bf16), V((GROUPS, cap, cols), bf16),
        V((GROUPS, 8, rows), f32), V((n_sp, 8, rows), f32),
        V((2, n_tp, n_z, cap, cols), bf16),
        V((width, ffw), bf16), V((width, ffw), bf16), V((ffw, width), bf16),
        V((half, ffw), bf16), V((n_tp, half, cols), f32),
        V((n_tp, half, cols), bf16), V((n_tp, half, cols), bf16),
        V((n_tp, half, cols), bf16), V((n_tp, half, cols), bf16),
        V((n_z, cap, cols), bf16), V((n_z, cap, cols), bf16),
        V((n_tp, rows // n_tp, cols), f32), V((n_tp, rows // n_tp, cols), f32),
        dma((6,)), dma((4, n_sp)), dma((4, n_sp)), dma((n_sp,)), dma((n_sp,)),
        dma((n_tp,)), dma((n_tp,)), dma((n_tp,)), dma((n_tp,)),
        dma((n_z,)), dma((n_z,)), dma((n_sp,)), dma((n_sp,)),
        dma((n_tp, n_z)), dma((n_tp, n_z)), dma((n_tp, n_z)), dma((n_tp, n_z)),
        dma((n_tp,)), dma((n_tp,)), dma((n_tp,)), dma((n_tp,)),
        dma((n_z,)), dma((n_z,)), dma((n_tp,)), dma((n_tp,)),
    ]
    dims = (n_sp, n_tp, rows, cols, cap, small_heads, hs, hl)
    return pl.pallas_call(
        functools.partial(fast_kernel, dims),
        out_shape=jax.ShapeDtypeStruct((rows // n_tp, width), bf16),
        in_specs=[vmem] * 7 + [hbm] * 3 + [vmem] * 6 + [hbm] * 3,
        out_specs=vmem,
        scratch_shapes=scratch,
        compiler_params=pltpu.CompilerParams(
            collective_id=0, has_side_effects=True, vmem_limit_bytes=60 * 1024 * 1024
        ),
        name="layer",
    )(
        query_small, key_small, value_small, query_large, key_large, value_large, bias,
        stream, out_small, out_large,
        gain_one[None], shift_one[None], gain_two[None], shift_two[None],
        expert_pick.T, route_weight.T, w_gate, w_up, w_down,
    )


def layer(*arrays):
    n_sp, n_tp = lax.axis_size("sp"), lax.axis_size("tp")
    heads = arrays[1].shape[1] // HEAD_SMALL + arrays[4].shape[1] // HEAD_LARGE
    experts = arrays[16].shape[0] * n_sp
    paired = experts == 2 * GROUPS and n_sp == experts
    if paired and heads == n_sp and arrays[7].shape[2] * 2 == n_sp and arrays[0].shape[1] % (128 * n_tp) == 0:
        return fast_local(*arrays)
    return local(*arrays)


def solution(mesh):
    placed = (
        P("sp", None),
        P("sp", "tp"),
        P("sp", "tp"),
        P("sp", "tp"),
        P("sp", "tp"),
        P("sp", "tp"),
        P("sp", "tp"),
        P("sp", None, "tp"),
        P("tp", None),
        P("tp", None),
        P(),
        P(),
        P(),
        P(),
        P("sp", None),
        P("sp", None),
        P("sp", None, "tp"),
        P("sp", None, "tp"),
        P("sp", "tp", None),
    )
    return jax.shard_map(
        layer, mesh=mesh, in_specs=placed, out_specs=P(("sp", "tp"), None), check_vma=False
    )
```

```python
import functools

import jax
import jax.numpy as jnp
from jax import lax
from jax.experimental import pallas as pl
from jax.experimental.pallas import tpu as pltpu
from jax.sharding import PartitionSpec as P

HEAD_SMALL = 64
HEAD_LARGE = 128


ALPHA_RES = 2.0**0.25
NORM_EPS = 1e-05


def layer_norm(inputs, gain_vec, shift_vec):
    average = jnp.mean(inputs, axis=-1, keepdims=True)
    centred = inputs - average
    variance = jnp.mean(centred * centred, axis=-1, keepdims=True)
    return centred * lax.rsqrt(variance + NORM_EPS) * gain_vec + shift_vec


def stick_group(queries, key_rows, value_rows, log_bias, position):
    query_count = queries.shape[0]
    head_count = queries.shape[1]
    value_size = value_rows.shape[2]
    key_span = 4 * query_count
    score_scale = queries.shape[2] ** (-0.5)
    query_pos = position * query_count + jnp.arange(query_count, dtype=jnp.int32)
    block_count = (position * query_count + query_count + key_span - 1) // key_span

    def visit_block(turn_index, carry):
        running, stay_sum = carry
        first_key = (block_count - 1 - turn_index) * key_span
        key_block = lax.dynamic_slice_in_dim(key_rows, first_key, key_span, 0)
        value_block = lax.dynamic_slice_in_dim(value_rows, first_key, key_span, 0)
        bias_block = lax.dynamic_slice_in_dim(log_bias, first_key, key_span, 0).astype(jnp.float32)
        scores = jnp.einsum("qhd,khd->hqk", queries, key_block, preferred_element_type=jnp.float32)
        scores = scores * score_scale + bias_block.T[:, None, :]
        key_pos = first_key + jnp.arange(key_span, dtype=jnp.int32)
        causal = (key_pos[None, :] < query_pos[:, None])[None]
        log_stay = jnp.where(causal, jax.nn.log_sigmoid(-scores), 0.0)
        later_sum = lax.cumsum(log_stay, axis=2, reverse=True) - log_stay + stay_sum[:, :, None]
        stick_weight = jnp.where(
            causal, jnp.exp(jax.nn.log_sigmoid(scores) + later_sum), 0.0
        ).astype(jnp.bfloat16)
        running = running + jnp.einsum(
            "hqk,khd->qhd", stick_weight, value_block, preferred_element_type=jnp.float32
        )
        stay_sum = stay_sum + jnp.sum(log_stay, axis=2)
        return (running, stay_sum)

    start_total = jnp.zeros((query_count, head_count, value_size), jnp.float32)
    start_stay = jnp.zeros((head_count, query_count), jnp.float32)
    running, stay_sum = lax.fori_loop(0, block_count, visit_block, (start_total, start_stay))
    return running.reshape(query_count, head_count * value_size).astype(jnp.bfloat16)


def split_heads(array, head_size):
    return array.reshape(array.shape[0], array.shape[1] // head_size, head_size)


def local(
    stream,
    query_small,
    key_small,
    value_small,
    query_large,
    key_large,
    value_large,
    key_bias,
    out_small,
    out_large,
    gain_one,
    shift_one,
    gain_two,
    shift_two,
    expert_pick,
    route_weight,
    w_gate,
    w_up,
    w_down,
):
    row_count = stream.shape[0]
    position = lax.axis_index("sp")
    gathered = (
        lax.all_gather(key_small, "sp", axis=0, tiled=True),
        lax.all_gather(value_small, "sp", axis=0, tiled=True),
        lax.all_gather(key_large, "sp", axis=0, tiled=True),
        lax.all_gather(value_large, "sp", axis=0, tiled=True),
        lax.all_gather(key_bias, "sp", axis=0, tiled=True),
    )
    att_small = stick_group(
        split_heads(query_small, HEAD_SMALL),
        split_heads(gathered[0], HEAD_SMALL),
        split_heads(gathered[1], HEAD_SMALL),
        gathered[4][:, 0],
        position,
    )
    att_large = stick_group(
        split_heads(query_large, HEAD_LARGE),
        split_heads(gathered[2], HEAD_LARGE),
        split_heads(gathered[3], HEAD_LARGE),
        gathered[4][:, 1],
        position,
    )
    partial_value = jnp.dot(att_small, out_small, preferred_element_type=jnp.float32)
    partial_value = partial_value + jnp.dot(
        att_large, out_large, preferred_element_type=jnp.float32
    )
    mixer_out = lax.psum(partial_value.astype(jnp.bfloat16), "tp").astype(jnp.float32)
    normed = layer_norm(
        ALPHA_RES * stream.astype(jnp.float32) + mixer_out, gain_one, shift_one
    ).astype(jnp.bfloat16)
    experts = w_gate.shape[0] * lax.axis_size("sp")
    capacity = 4 * row_count // experts
    tp_count = lax.axis_size("tp")
    tp_index = lax.axis_index("tp")
    per_lane = capacity // tp_count
    flat_picks = expert_pick.reshape(-1)
    one_hot = (flat_picks[:, None] == jnp.arange(experts, dtype=jnp.int32)[None, :]).astype(
        jnp.int32
    )
    slot_rank = jnp.sum((jnp.cumsum(one_hot, axis=0) - one_hot) * one_hot, axis=1)
    slot_index = (flat_picks * capacity + slot_rank).reshape(row_count, 2)

    def selector(first_slot, slot_count):
        target = (
            jnp.arange(experts, dtype=jnp.int32)[:, None] * capacity
            + first_slot
            + jnp.arange(slot_count, dtype=jnp.int32)[None, :]
        ).reshape(-1)
        return [target[:, None] == slot_index[None, :, pick_index] for pick_index in range(2)]

    own_select = selector(tp_index * per_lane, per_lane)
    all_select = selector(0, capacity)
    placing = (all_select[0] | all_select[1]).astype(jnp.bfloat16)
    outgoing = jnp.dot(placing, normed, preferred_element_type=jnp.float32).astype(jnp.bfloat16)
    arrived = lax.all_to_all(
        outgoing.reshape(experts, capacity, normed.shape[1]),
        "sp",
        split_axis=0,
        concat_axis=0,
        tiled=True,
    )
    flat_rows = arrived.reshape(-1, arrived.shape[2])
    gate = jnp.dot(flat_rows, w_gate[0], preferred_element_type=jnp.float32)
    upper = jnp.dot(flat_rows, w_up[0], preferred_element_type=jnp.float32)
    hidden = (jax.nn.silu(gate) * upper).astype(jnp.bfloat16)
    expert_terms = jnp.dot(hidden, w_down[0], preferred_element_type=jnp.float32).reshape(
        arrived.shape
    )
    summed = lax.psum_scatter(
        expert_terms.astype(jnp.bfloat16), "tp", scatter_dimension=1, tiled=True
    )
    returned = lax.all_to_all(summed, "sp", split_axis=0, concat_axis=0, tiled=True).reshape(
        experts * per_lane, normed.shape[1]
    )
    picked_first = jnp.einsum(
        "sr,sd->rd",
        own_select[0].astype(jnp.bfloat16),
        returned,
        preferred_element_type=jnp.float32,
    )
    picked_second = jnp.einsum(
        "sr,sd->rd",
        own_select[1].astype(jnp.bfloat16),
        returned,
        preferred_element_type=jnp.float32,
    )
    partial_mix = route_weight[:, 0:1] * picked_first + route_weight[:, 1:2] * picked_second
    expert_mix = lax.psum_scatter(
        partial_mix.astype(jnp.bfloat16), "tp", scatter_dimension=0, tiled=True
    ).astype(jnp.float32)
    own_count = row_count // tp_count
    own_rows = lax.dynamic_slice_in_dim(normed, tp_index * own_count, own_count, 0).astype(
        jnp.float32
    )
    return layer_norm(ALPHA_RES * own_rows + expert_mix, gain_two, shift_two).astype(jnp.bfloat16)


GROUPS = 4


def fast_kernel(
    dims,
    qs_ref, ks_ref, vs_ref, ql_ref, kl_ref, vl_ref, bias_ref, stream_ref, os_ref, ol_ref,
    g1_ref, b1_ref, g2_ref, b2_ref, pick_ref, route_ref, wg_ref, wu_ref, wd_ref,
    out_ref,
    pack_a, pack_v, rq, rk, rv, rb, aq, ak, ao, ra, wos, wol, strm, pb, rp, st, rst, normed,
    place, xs, wsend, wrecv, ag, wg, wu, wd, hid, own_y, cs, cr, ts, rr, zs, zr, fs, fr,
    load_sem, q_send, q_recv, a_send, a_recv, p_send, p_recv, s_send, s_recv,
    x_send, x_recv, w_send, w_recv, g_send, g_recv, h_send, h_recv, c_send, c_recv,
    t_send, t_recv, z_send, z_recv, f_send, f_recv,
):
    n_sp, n_tp, rows, cols, cap, small_heads, hs, hl = dims
    f32, bf16 = jnp.float32, jnp.bfloat16
    sp = lax.axis_index("sp")
    tp = lax.axis_index("tp")
    core = lax.rem(sp, 2)
    chip = lax.div(sp, 2)
    sibling = sp + 1 - 2 * core
    n_z = n_sp // 2
    is_small = sp < small_heads
    large_heads = n_sp - small_heads
    ffw = wg_ref.shape[2]
    width = n_tp * cols

    def mesh_copy(src, dst, send, recv, target):
        return pltpu.make_async_remote_copy(
            src_ref=src, dst_ref=dst, send_sem=send, recv_sem=recv,
            device_id=target, device_id_type=pl.DeviceIdType.MESH,
        )

    def sp_at(j):
        return (j, tp)

    def tp_at(j):
        return (sp, j)

    def flip(index, mask, count):
        total, bit = 0, 1
        while bit < count:
            digit = lax.rem(lax.div(index, bit), 2)
            total = total + bit * (1 - digit if mask & bit else digit)
            bit *= 2
        return total

    z_masks = [*range(0, n_z, 2), *range(1, n_z, 2)]
    z_order = [flip(chip, m, n_z) for m in z_masks]
    peers = [flip(tp, m, n_tp) for m in range(n_tp)]
    out_peers = [*peers[:0:-1], peers[0]]

    barrier = pltpu.get_barrier_semaphore()
    for k in range(1, n_sp):
        pl.semaphore_signal(barrier, inc=1, device_id=sp_at(lax.rem(sp + k, n_sp)), device_id_type=pl.DeviceIdType.MESH)
    for k in range(1, n_tp):
        pl.semaphore_signal(barrier, inc=1, device_id=tp_at(lax.rem(tp + k, n_tp)), device_id_type=pl.DeviceIdType.MESH)

    own_cols = pl.ds(pl.multiple_of(tp * cols, cols), cols)
    loads = [
        pltpu.make_async_copy(os_ref, wos, load_sem.at[0]),
        pltpu.make_async_copy(ol_ref, wol, load_sem.at[1]),
        pltpu.make_async_copy(stream_ref.at[:, own_cols], strm, load_sem.at[2]),
        pltpu.make_async_copy(wg_ref.at[0], wg, load_sem.at[3]),
        pltpu.make_async_copy(wu_ref.at[0], wu, load_sem.at[4]),
        pltpu.make_async_copy(wd_ref.at[0], wd, load_sem.at[5]),
    ]
    for load in loads:
        load.start()

    for h in range(small_heads):
        part = slice(h * hs, (h + 1) * hs)
        pack_a[h] = jnp.concatenate([qs_ref[:, part], ks_ref[:, part]], axis=1)
        pack_v[h] = jnp.concatenate([vs_ref[:, part], jnp.zeros((rows, hl - hs), bf16)], axis=1)

    pl.semaphore_wait(barrier, n_sp + n_tp - 2)

    def head_copies(j, slot):
        if j < small_heads:
            pairs = [(0, pack_a.at[j], rq), (2, pack_v.at[j], rv)]
        else:
            part = pl.ds((j - small_heads) * hl, hl)
            pairs = [(0, ql_ref.at[:, part], rq), (1, kl_ref.at[:, part], rk), (2, vl_ref.at[:, part], rv)]
        pairs.append((3, bias_ref.at[j], rb))
        return [(kind, src, dst.at[slot]) for kind, src, dst in pairs]

    for j in range(n_sp):
        @pl.when(j != sp)
        def _():
            for kind, src, dst in head_copies(j, sp):
                mesh_copy(src, dst, q_send.at[kind, j], q_recv.at[kind, sp], sp_at(j)).start()

        @pl.when(j == sp)
        def _():
            for kind, src, dst in head_copies(j, j):
                pltpu.make_async_copy(src, dst, q_recv.at[kind, j]).start()

    group = lax.div(pick_ref[0:1, :], 2)
    first_even = lax.rem(pick_ref[0:1, :], 2) == 0
    sub8 = lax.broadcasted_iota(jnp.int32, (8, rows), 0)
    one_hot = (sub8 == group).astype(f32)
    sub_r = lax.broadcasted_iota(jnp.int32, (rows, rows), 0)
    lane_r = lax.broadcasted_iota(jnp.int32, (rows, rows), 1)
    before = (sub_r < lane_r).astype(f32).astype(bf16)
    counts = jnp.dot(one_hot.astype(bf16), before, preferred_element_type=f32)
    rank = jnp.sum(one_hot * counts, axis=0, keepdims=True).astype(jnp.int32)
    slot_row = group * cap + rank
    slot_iota = lax.broadcasted_iota(jnp.int32, (GROUPS * cap, rows), 0)
    place[...] = (slot_iota == slot_row).astype(f32).astype(bf16)
    w_even = jnp.where(first_even, route_ref[0:1, :], route_ref[1:2, :])
    w_odd = jnp.where(first_even, route_ref[1:2, :], route_ref[0:1, :])
    w8 = jnp.where(sub8 == 0, w_even, jnp.where(sub8 == 1, w_odd, 0.0))
    w_hi = w8.astype(bf16)
    w_lo = (w8 - w_hi.astype(f32)).astype(bf16)
    for g in range(GROUPS):
        pick_g = ((sub_r == slot_row - g * cap) & (sub_r < cap)).astype(f32).astype(bf16)
        last = (((1,), (1,)), ((), ()))
        wsend[g] = lax.dot_general(w_hi, pick_g, last, preferred_element_type=f32) + lax.dot_general(
            w_lo, pick_g, last, preferred_element_type=f32
        )

    for j in range(n_sp):
        for kind in (0, 2, 3):
            dst = (rq, None, rv, rb)[kind].at[j]
            pltpu.make_async_copy(dst, dst, q_recv.at[kind, j]).wait()

    @pl.when(jnp.logical_not(is_small))
    def _():
        for j in range(n_sp):
            pltpu.make_async_copy(rk.at[j], rk.at[j], q_recv.at[1, j]).wait()
            aq[pl.ds(j * rows, rows), :] = rq[j]
            ak[pl.ds(j * rows, rows), :] = rk[j]

    @pl.when(is_small)
    def _():
        lane = lax.broadcasted_iota(jnp.int32, (rows, hl), 1)
        for j in range(n_sp):
            both = rq[j]
            aq[pl.ds(j * rows, rows), :] = jnp.where(lane < hs, both, jnp.zeros_like(both))
            ak[pl.ds(j * rows, rows), :] = jnp.concatenate([both[:, hs:], both[:, :hs]], axis=1)

    for j in range(n_sp):
        @pl.when(j != sp)
        def _():
            for kind, src, dst in head_copies(j, sp):
                mesh_copy(src, dst, q_send.at[kind, j], q_recv.at[kind, sp], sp_at(j)).wait_send()

    scale = jnp.where(is_small, hs**-0.5, hl**-0.5).astype(f32)
    span = 2 * rows
    sub_t = lax.broadcasted_iota(jnp.int32, (span, span), 0)
    lane_t = lax.broadcasted_iota(jnp.int32, (span, span), 1)
    tri = (sub_t >= lane_t).astype(f32).astype(bf16)
    causal = lane_t < sub_t

    def tile(query, kj, diagonal, total, later):
        keys = ak[pl.ds(pl.multiple_of(kj * span, span), span), :]
        log_odds = jnp.concatenate([rb[2 * kj, 0:1, :], rb[2 * kj + 1, 0:1, :]], axis=1)
        score = lax.dot_general(query, keys, (((1,), (1,)), ((), ())), preferred_element_type=f32)
        score = score * scale + log_odds
        soft = jnp.maximum(score, 0.0) + jnp.log(1.0 + jnp.exp(-jnp.abs(score)))
        if diagonal:
            soft = jnp.where(causal, soft, 0.0)
        high = soft.astype(bf16)
        low = (soft - high.astype(f32)).astype(bf16)
        run = jnp.dot(high, tri, preferred_element_type=f32) + jnp.dot(low, tri, preferred_element_type=f32)
        stick = jnp.exp(score - run - later)
        if diagonal:
            stick = jnp.where(causal, stick, 0.0)
        values = jnp.concatenate([rv[2 * kj], rv[2 * kj + 1]], axis=0)
        total = total + jnp.dot(stick.astype(bf16), values, preferred_element_type=f32)
        return total, later + run[:, 0:1]

    for qi in range(n_sp // 2):
        query = aq[qi * span:(qi + 1) * span, :]
        carry = tile(query, qi, True, jnp.zeros((span, hl), f32), jnp.zeros((span, 1), f32))
        if qi:
            def visit(turn, carry):
                return tile(query, qi - 1 - turn, False, *carry)
            carry = lax.fori_loop(0, qi, visit, carry)
        for half in range(2):
            d = 2 * qi + half
            ao[d] = carry[0][half * rows:(half + 1) * rows].astype(bf16)
        for half in range(2):
            d = 2 * qi + half

            @pl.when(d != sp)
            def _():
                mesh_copy(ao.at[d], ra.at[sp], a_send.at[d], a_recv.at[sp], sp_at(d)).start()

            @pl.when(d == sp)
            def _():
                pltpu.make_async_copy(ao.at[d], ra.at[d], a_recv.at[d]).start()

    for load in loads[:3]:
        load.wait()
    for j in range(n_sp):
        pltpu.make_async_copy(ra.at[j], ra.at[j], a_recv.at[j]).wait()
    att_small = jnp.concatenate([ra[j][:, :hs] for j in range(small_heads)], axis=1)
    att_large = jnp.concatenate([ra[j] for j in range(small_heads, n_sp)], axis=1)

    def tp_wait_recv(buf, sem, src):
        pltpu.make_async_copy(buf.at[src], buf.at[src], sem.at[src]).wait()

    for k in range(1, n_tp + 1):
        t = lax.rem(tp + k, n_tp)
        part = pl.ds(pl.multiple_of(t * cols, cols), cols)
        term = jnp.dot(att_small, wos[:, part], preferred_element_type=f32)
        term = term + jnp.dot(att_large, wol[:, part], preferred_element_type=f32)
        pb[k - 1] = term.astype(bf16)
        if k < n_tp:
            mesh_copy(pb.at[k - 1], rp.at[tp], p_send.at[k], p_recv.at[tp], tp_at(t)).start()
    mixed = ALPHA_RES * strm[...].astype(f32) + pb[n_tp - 1].astype(f32)
    for k in range(1, n_tp):
        src = lax.rem(tp + k, n_tp)
        tp_wait_recv(rp, p_recv, src)
        mixed = mixed + rp[src].astype(f32)

    eye = sub_r == lane_r

    def to_row(column):
        return jnp.sum(jnp.where(eye, column, 0.0), axis=0, keepdims=True)

    def to_column(row):
        return jnp.sum(jnp.where(eye, row, 0.0), axis=1, keepdims=True)

    own_mean = jnp.mean(mixed, axis=1, keepdims=True)
    centred = mixed - own_mean
    own_square = jnp.sum(centred * centred, axis=1, keepdims=True)
    mean_row, square_row = to_row(own_mean), to_row(own_square)
    st[...] = jnp.where(sub8 == 0, mean_row, square_row)
    for k in range(1, n_tp):
        t = lax.rem(tp + k, n_tp)
        mesh_copy(st, rst.at[tp], s_send.at[k], s_recv.at[tp], tp_at(t)).start()
    means, squares = [mean_row], [square_row]
    for k in range(1, n_tp):
        src = lax.rem(tp + k, n_tp)
        tp_wait_recv(rst, s_recv, src)
        means.append(rst[src, 0:1, :])
        squares.append(rst[src, 1:2, :])
    full_mean = sum(means) / n_tp
    spread = sum(squares) + cols * sum((m - full_mean) * (m - full_mean) for m in means)
    scale_row = lax.rsqrt(spread / width + NORM_EPS)
    norm_val = (mixed - to_column(full_mean)) * to_column(scale_row) * g1_ref[:, own_cols] + b1_ref[:, own_cols]
    normed[...] = norm_val.astype(bf16)

    for g in range(GROUPS):
        xs[g] = jnp.dot(place[g * cap:(g + 1) * cap, :], normed[...], preferred_element_type=f32).astype(bf16)
    for k in range(n_z):
        g = z_order[k]
        dst = ag.at[core, tp, chip]
        if k == 0:
            pltpu.make_async_copy(xs.at[g], dst, x_recv.at[chip]).start()
        else:
            mesh_copy(xs.at[g], dst, x_send.at[k], x_recv.at[chip], sp_at(2 * g + core)).start()
    for k in range(n_sp):
        j = lax.rem(sp + k, n_sp)
        if k == 0:
            pltpu.make_async_copy(wsend.at[chip], wrecv.at[sp], w_recv.at[sp]).start()
        else:
            mesh_copy(wsend.at[lax.div(j, 2)], wrecv.at[sp], w_send.at[k], w_recv.at[sp], sp_at(j)).start()

    for z in z_order:
        piece = ag.at[core, tp, z]
        pltpu.make_async_copy(piece, piece, x_recv.at[z]).wait()
        for m in range(1, n_tp):
            mesh_copy(piece, piece, g_send.at[m, z], g_recv.at[tp, z], tp_at(peers[m])).start()
        mesh_copy(piece, piece, h_send.at[tp, z], h_recv.at[tp, z], sp_at(sibling)).start()
    for j in range(n_sp):
        pltpu.make_async_copy(wrecv.at[j], wrecv.at[j], w_recv.at[j]).wait()
    for load in loads[3:]:
        load.wait()

    other = 1 - core
    lane_c = lax.broadcasted_iota(jnp.int32, (cap, rows), 1)
    sub_c = lax.broadcasted_iota(jnp.int32, (cap, rows), 0)
    step = min(256, ffw)
    half = (n_z // 2) * cap

    def slot_weights(c, z):
        row = wrecv[2 * z + c, pl.ds(core, 1), :]
        return jnp.sum(jnp.where(sub_c == lane_c, row, 0.0), axis=1, keepdims=True)

    for p in range(2):
        zs_p = z_order[p * (n_z // 2):(p + 1) * (n_z // 2)]
        for z in zs_p:
            for m in range(1, n_tp):
                piece = ag.at[core, peers[m], z]
                pltpu.make_async_copy(piece, piece, g_recv.at[peers[m], z]).wait()
                mesh_copy(piece, piece, h_send.at[peers[m], z], h_recv.at[peers[m], z], sp_at(sibling)).start()
        for z in zs_p:
            for t in range(n_tp):
                piece = ag.at[other, t, z]
                pltpu.make_async_copy(piece, piece, h_recv.at[t, z]).wait()
        weights = jnp.concatenate([slot_weights(c, z) for c in (other, core) for z in zs_p], axis=0)

        def body(n, carry):
            part = pl.ds(pl.multiple_of(n * step, step), step)
            gate = jnp.zeros((2 * half, step), f32)
            upper = jnp.zeros((2 * half, step), f32)
            for t in range(n_tp):
                x = jnp.concatenate([ag[c, t, z] for c in (other, core) for z in zs_p], axis=0)
                gate = gate + jnp.dot(x, wg[t * cols:(t + 1) * cols, part], preferred_element_type=f32)
                upper = upper + jnp.dot(x, wu[t * cols:(t + 1) * cols, part], preferred_element_type=f32)
            hid[:, part] = (gate / (1.0 + jnp.exp(-gate)) * upper).astype(bf16)
            return carry

        lax.fori_loop(0, ffw // step, body, 0)

        def join(k):
            pltpu.make_async_copy(cr.at[p, k], cr.at[p, k], c_recv.at[p, k]).wait()
            both = own_y[p, k] + cr[p, k].astype(f32)
            if k == n_tp - 1:
                own_y[p, k] = both
                return
            for i in range(n_z // 2):
                kz = p * (n_z // 2) + i
                ts[k, kz] = both[i * cap:(i + 1) * cap].astype(bf16)
                mesh_copy(
                    ts.at[k, kz], rr.at[tp, kz], t_send.at[k, kz], t_recv.at[tp, kz], tp_at(out_peers[k])
                ).start()

        for k in range(n_tp):
            part = pl.ds(pl.multiple_of(out_peers[k] * cols, cols), cols)
            y = jnp.dot(hid[...], wd[:, part], preferred_element_type=f32) * weights
            cs[p, k] = y[:half].astype(bf16)
            mesh_copy(cs.at[p, k], cr.at[p, k], c_send.at[p, k], c_recv.at[p, k], sp_at(sibling)).start()
            own_y[p, k] = y[half:]
            if k:
                join(k - 1)
        join(n_tp - 1)

    for kz in range(n_z):
        z = z_order[kz]
        i = kz % (n_z // 2)
        total = own_y[kz // (n_z // 2), n_tp - 1, i * cap:(i + 1) * cap, :]
        for m in range(1, n_tp):
            src = peers[m]
            pltpu.make_async_copy(rr.at[src, kz], rr.at[src, kz], t_recv.at[src, kz]).wait()
            total = total + rr[src, kz].astype(f32)
        zs[kz] = total.astype(bf16)
        if kz:
            mesh_copy(zs.at[kz], zr.at[chip], z_send.at[kz], z_recv.at[chip], sp_at(2 * z + core)).start()
        else:
            pltpu.make_async_copy(zs.at[kz], zr.at[chip], z_recv.at[chip]).start()
    for z in range(n_z):
        pltpu.make_async_copy(zr.at[z], zr.at[z], z_recv.at[z]).wait()
    expert_mix = lax.dot_general(
        place[...], zr[...].reshape(n_z * cap, cols), (((0,), (0,)), ((), ())), preferred_element_type=f32
    )
    final = ALPHA_RES * normed[...].astype(f32) + expert_mix
    own_rows = rows // n_tp
    for t in range(n_tp):
        fs[t] = final[t * own_rows:(t + 1) * own_rows]
    for k in range(1, n_tp):
        t = lax.rem(tp + k, n_tp)
        mesh_copy(fs.at[t], fr.at[tp], f_send.at[k], f_recv.at[tp], tp_at(t)).start()
    keep = pltpu.make_async_copy(fs.at[tp], fr.at[tp], f_recv.at[tp])
    keep.start()
    for t in range(n_tp):
        tp_wait_recv(fr, f_recv, t)
    blocks = [fr[t] for t in range(n_tp)]
    average = sum(jnp.sum(b, axis=1, keepdims=True) for b in blocks) / width
    blocks = [b - average for b in blocks]
    variance = sum(jnp.sum(b * b, axis=1, keepdims=True) for b in blocks) / width
    inverse = lax.rsqrt(variance + NORM_EPS)
    for t in range(n_tp):
        part = slice(t * cols, (t + 1) * cols)
        out_ref[:, part] = (blocks[t] * inverse * g2_ref[:, part] + b2_ref[:, part]).astype(bf16)

    for d in range(n_sp):
        @pl.when(d != sp)
        def _():
            mesh_copy(ao.at[d], ra.at[sp], a_send.at[d], a_recv.at[sp], sp_at(d)).wait_send()
    for k in range(1, n_sp):
        j = lax.rem(sp + k, n_sp)
        mesh_copy(wsend.at[lax.div(j, 2)], wrecv.at[sp], w_send.at[k], w_recv.at[sp], sp_at(j)).wait_send()
    for k in range(1, n_tp):
        t = lax.rem(tp + k, n_tp)
        mesh_copy(pb.at[k - 1], rp.at[tp], p_send.at[k], p_recv.at[tp], tp_at(t)).wait_send()
        mesh_copy(st, rst.at[tp], s_send.at[k], s_recv.at[tp], tp_at(t)).wait_send()
        mesh_copy(fs.at[t], fr.at[tp], f_send.at[k], f_recv.at[tp], tp_at(t)).wait_send()
        for z in range(n_z):
            piece = ag.at[core, tp, z]
            mesh_copy(piece, piece, g_send.at[k, z], g_recv.at[tp, z], tp_at(peers[k])).wait_send()
            mesh_copy(
                ts.at[k - 1, z], rr.at[tp, z], t_send.at[k - 1, z], t_recv.at[tp, z], tp_at(out_peers[k - 1])
            ).wait_send()
    for k in range(1, n_z):
        g = z_order[k]
        mesh_copy(xs.at[g], ag.at[core, tp, chip], x_send.at[k], x_recv.at[chip], sp_at(2 * g + core)).wait_send()
        mesh_copy(zs.at[k], zr.at[chip], z_send.at[k], z_recv.at[chip], sp_at(2 * g + core)).wait_send()
    for t in range(n_tp):
        for p in range(2):
            mesh_copy(cs.at[p, t], cr.at[p, t], c_send.at[p, t], c_recv.at[p, t], sp_at(sibling)).wait_send()
        for z in range(n_z):
            piece = ag.at[core, t, z]
            mesh_copy(piece, piece, h_send.at[t, z], h_recv.at[t, z], sp_at(sibling)).wait_send()


def fast_local(
    stream, query_small, key_small, value_small, query_large, key_large, value_large, key_bias,
    out_small, out_large, gain_one, shift_one, gain_two, shift_two, expert_pick, route_weight,
    w_gate, w_up, w_down,
):
    f32, bf16 = jnp.float32, jnp.bfloat16
    n_sp, n_tp = lax.axis_size("sp"), lax.axis_size("tp")
    rows, width = stream.shape
    cols = width // n_tp
    hs, hl = HEAD_SMALL, HEAD_LARGE
    small_heads = query_small.shape[1] // hs
    cap = 4 * rows // (w_gate.shape[0] * n_sp)
    n_z = n_sp // 2
    ffw = w_gate.shape[2]
    bias = key_bias.astype(f32).transpose(1, 2, 0).reshape(n_sp, 1, rows)
    bias = jnp.broadcast_to(bias, (n_sp, 8, rows))
    vmem = pl.BlockSpec(memory_space=pltpu.VMEM)
    hbm = pl.BlockSpec(memory_space=pl.ANY)
    dma = pltpu.SemaphoreType.DMA
    V = pltpu.VMEM
    half = n_z * cap
    scratch = [
        V((small_heads, rows, hl), bf16), V((small_heads, rows, hl), bf16),
        V((n_sp, rows, hl), bf16), V((n_sp, rows, hl), bf16), V((n_sp, rows, hl), bf16),
        V((n_sp, 8, rows), f32),
        V((n_sp * rows, hl), bf16), V((n_sp * rows, hl), bf16),
        V((n_sp, rows, hl), bf16), V((n_sp, rows, hl), bf16),
        V(out_small.shape, bf16), V(out_large.shape, bf16), V((rows, cols), bf16),
        V((n_tp, rows, cols), bf16), V((n_tp, rows, cols), bf16),
        V((8, rows), f32), V((n_tp, 8, rows), f32), V((rows, cols), bf16),
        V((GROUPS * cap, rows), bf16), V((GROUPS, cap, cols), bf16),
        V((GROUPS, 8, rows), f32), V((n_sp, 8, rows), f32),
        V((2, n_tp, n_z, cap, cols), bf16),
        V((width, ffw), bf16), V((width, ffw), bf16), V((ffw, width), bf16),
        V((half, ffw), bf16), V((2, n_tp, half // 2, cols), f32),
        V((2, n_tp, half // 2, cols), bf16), V((2, n_tp, half // 2, cols), bf16),
        V((n_tp - 1, n_z, cap, cols), bf16), V((n_tp, n_z, cap, cols), bf16),
        V((n_z, cap, cols), bf16), V((n_z, cap, cols), bf16),
        V((n_tp, rows // n_tp, cols), f32), V((n_tp, rows // n_tp, cols), f32),
        dma((6,)), dma((4, n_sp)), dma((4, n_sp)), dma((n_sp,)), dma((n_sp,)),
        dma((n_tp,)), dma((n_tp,)), dma((n_tp,)), dma((n_tp,)),
        dma((n_z,)), dma((n_z,)), dma((n_sp,)), dma((n_sp,)),
        dma((n_tp, n_z)), dma((n_tp, n_z)), dma((n_tp, n_z)), dma((n_tp, n_z)),
        dma((2, n_tp)), dma((2, n_tp)), dma((n_tp, n_z)), dma((n_tp, n_z)),
        dma((n_z,)), dma((n_z,)), dma((n_tp,)), dma((n_tp,)),
    ]
    dims = (n_sp, n_tp, rows, cols, cap, small_heads, hs, hl)
    return pl.pallas_call(
        functools.partial(fast_kernel, dims),
        out_shape=jax.ShapeDtypeStruct((rows // n_tp, width), bf16),
        in_specs=[vmem] * 7 + [hbm] * 3 + [vmem] * 6 + [hbm] * 3,
        out_specs=vmem,
        scratch_shapes=scratch,
        compiler_params=pltpu.CompilerParams(
            collective_id=0, has_side_effects=True, vmem_limit_bytes=60 * 1024 * 1024
        ),
        name="layer",
    )(
        query_small, key_small, value_small, query_large, key_large, value_large, bias,
        stream, out_small, out_large,
        gain_one[None], shift_one[None], gain_two[None], shift_two[None],
        expert_pick.T, route_weight.T, w_gate, w_up, w_down,
    )


def layer(*arrays):
    n_sp, n_tp = lax.axis_size("sp"), lax.axis_size("tp")
    heads = arrays[1].shape[1] // HEAD_SMALL + arrays[4].shape[1] // HEAD_LARGE
    experts = arrays[16].shape[0] * n_sp
    paired = experts == 2 * GROUPS and n_sp == experts
    if paired and heads == n_sp and arrays[7].shape[2] * 2 == n_sp and arrays[0].shape[1] % (128 * n_tp) == 0:
        return fast_local(*arrays)
    return local(*arrays)


def solution(mesh):
    placed = (
        P("sp", None),
        P("sp", "tp"),
        P("sp", "tp"),
        P("sp", "tp"),
        P("sp", "tp"),
        P("sp", "tp"),
        P("sp", "tp"),
        P("sp", None, "tp"),
        P("tp", None),
        P("tp", None),
        P(),
        P(),
        P(),
        P(),
        P("sp", None),
        P("sp", None),
        P("sp", None, "tp"),
        P("sp", None, "tp"),
        P("sp", "tp", None),
    )
    return jax.shard_map(
        layer, mesh=mesh, in_specs=placed, out_specs=P(("sp", "tp"), None), check_vma=False
    )
```

```python
import functools

import jax
import jax.numpy as jnp
from jax import lax
from jax.experimental import pallas as pl
from jax.experimental.pallas import tpu as pltpu
from jax.sharding import PartitionSpec as P

HEAD_SMALL = 64
HEAD_LARGE = 128


ALPHA_RES = 2.0**0.25
NORM_EPS = 1e-05


def layer_norm(inputs, gain_vec, shift_vec):
    average = jnp.mean(inputs, axis=-1, keepdims=True)
    centred = inputs - average
    variance = jnp.mean(centred * centred, axis=-1, keepdims=True)
    return centred * lax.rsqrt(variance + NORM_EPS) * gain_vec + shift_vec


def stick_group(queries, key_rows, value_rows, log_bias, position):
    query_count = queries.shape[0]
    head_count = queries.shape[1]
    value_size = value_rows.shape[2]
    key_span = 4 * query_count
    score_scale = queries.shape[2] ** (-0.5)
    query_pos = position * query_count + jnp.arange(query_count, dtype=jnp.int32)
    block_count = (position * query_count + query_count + key_span - 1) // key_span

    def visit_block(turn_index, carry):
        running, stay_sum = carry
        first_key = (block_count - 1 - turn_index) * key_span
        key_block = lax.dynamic_slice_in_dim(key_rows, first_key, key_span, 0)
        value_block = lax.dynamic_slice_in_dim(value_rows, first_key, key_span, 0)
        bias_block = lax.dynamic_slice_in_dim(log_bias, first_key, key_span, 0).astype(jnp.float32)
        scores = jnp.einsum("qhd,khd->hqk", queries, key_block, preferred_element_type=jnp.float32)
        scores = scores * score_scale + bias_block.T[:, None, :]
        key_pos = first_key + jnp.arange(key_span, dtype=jnp.int32)
        causal = (key_pos[None, :] < query_pos[:, None])[None]
        log_stay = jnp.where(causal, jax.nn.log_sigmoid(-scores), 0.0)
        later_sum = lax.cumsum(log_stay, axis=2, reverse=True) - log_stay + stay_sum[:, :, None]
        stick_weight = jnp.where(
            causal, jnp.exp(jax.nn.log_sigmoid(scores) + later_sum), 0.0
        ).astype(jnp.bfloat16)
        running = running + jnp.einsum(
            "hqk,khd->qhd", stick_weight, value_block, preferred_element_type=jnp.float32
        )
        stay_sum = stay_sum + jnp.sum(log_stay, axis=2)
        return (running, stay_sum)

    start_total = jnp.zeros((query_count, head_count, value_size), jnp.float32)
    start_stay = jnp.zeros((head_count, query_count), jnp.float32)
    running, stay_sum = lax.fori_loop(0, block_count, visit_block, (start_total, start_stay))
    return running.reshape(query_count, head_count * value_size).astype(jnp.bfloat16)


def split_heads(array, head_size):
    return array.reshape(array.shape[0], array.shape[1] // head_size, head_size)


def local(
    stream,
    query_small,
    key_small,
    value_small,
    query_large,
    key_large,
    value_large,
    key_bias,
    out_small,
    out_large,
    gain_one,
    shift_one,
    gain_two,
    shift_two,
    expert_pick,
    route_weight,
    w_gate,
    w_up,
    w_down,
):
    row_count = stream.shape[0]
    position = lax.axis_index("sp")
    gathered = (
        lax.all_gather(key_small, "sp", axis=0, tiled=True),
        lax.all_gather(value_small, "sp", axis=0, tiled=True),
        lax.all_gather(key_large, "sp", axis=0, tiled=True),
        lax.all_gather(value_large, "sp", axis=0, tiled=True),
        lax.all_gather(key_bias, "sp", axis=0, tiled=True),
    )
    att_small = stick_group(
        split_heads(query_small, HEAD_SMALL),
        split_heads(gathered[0], HEAD_SMALL),
        split_heads(gathered[1], HEAD_SMALL),
        gathered[4][:, 0],
        position,
    )
    att_large = stick_group(
        split_heads(query_large, HEAD_LARGE),
        split_heads(gathered[2], HEAD_LARGE),
        split_heads(gathered[3], HEAD_LARGE),
        gathered[4][:, 1],
        position,
    )
    partial_value = jnp.dot(att_small, out_small, preferred_element_type=jnp.float32)
    partial_value = partial_value + jnp.dot(
        att_large, out_large, preferred_element_type=jnp.float32
    )
    mixer_out = lax.psum(partial_value.astype(jnp.bfloat16), "tp").astype(jnp.float32)
    normed = layer_norm(
        ALPHA_RES * stream.astype(jnp.float32) + mixer_out, gain_one, shift_one
    ).astype(jnp.bfloat16)
    experts = w_gate.shape[0] * lax.axis_size("sp")
    capacity = 4 * row_count // experts
    tp_count = lax.axis_size("tp")
    tp_index = lax.axis_index("tp")
    per_lane = capacity // tp_count
    flat_picks = expert_pick.reshape(-1)
    one_hot = (flat_picks[:, None] == jnp.arange(experts, dtype=jnp.int32)[None, :]).astype(
        jnp.int32
    )
    slot_rank = jnp.sum((jnp.cumsum(one_hot, axis=0) - one_hot) * one_hot, axis=1)
    slot_index = (flat_picks * capacity + slot_rank).reshape(row_count, 2)

    def selector(first_slot, slot_count):
        target = (
            jnp.arange(experts, dtype=jnp.int32)[:, None] * capacity
            + first_slot
            + jnp.arange(slot_count, dtype=jnp.int32)[None, :]
        ).reshape(-1)
        return [target[:, None] == slot_index[None, :, pick_index] for pick_index in range(2)]

    own_select = selector(tp_index * per_lane, per_lane)
    all_select = selector(0, capacity)
    placing = (all_select[0] | all_select[1]).astype(jnp.bfloat16)
    outgoing = jnp.dot(placing, normed, preferred_element_type=jnp.float32).astype(jnp.bfloat16)
    arrived = lax.all_to_all(
        outgoing.reshape(experts, capacity, normed.shape[1]),
        "sp",
        split_axis=0,
        concat_axis=0,
        tiled=True,
    )
    flat_rows = arrived.reshape(-1, arrived.shape[2])
    gate = jnp.dot(flat_rows, w_gate[0], preferred_element_type=jnp.float32)
    upper = jnp.dot(flat_rows, w_up[0], preferred_element_type=jnp.float32)
    hidden = (jax.nn.silu(gate) * upper).astype(jnp.bfloat16)
    expert_terms = jnp.dot(hidden, w_down[0], preferred_element_type=jnp.float32).reshape(
        arrived.shape
    )
    summed = lax.psum_scatter(
        expert_terms.astype(jnp.bfloat16), "tp", scatter_dimension=1, tiled=True
    )
    returned = lax.all_to_all(summed, "sp", split_axis=0, concat_axis=0, tiled=True).reshape(
        experts * per_lane, normed.shape[1]
    )
    picked_first = jnp.einsum(
        "sr,sd->rd",
        own_select[0].astype(jnp.bfloat16),
        returned,
        preferred_element_type=jnp.float32,
    )
    picked_second = jnp.einsum(
        "sr,sd->rd",
        own_select[1].astype(jnp.bfloat16),
        returned,
        preferred_element_type=jnp.float32,
    )
    partial_mix = route_weight[:, 0:1] * picked_first + route_weight[:, 1:2] * picked_second
    expert_mix = lax.psum_scatter(
        partial_mix.astype(jnp.bfloat16), "tp", scatter_dimension=0, tiled=True
    ).astype(jnp.float32)
    own_count = row_count // tp_count
    own_rows = lax.dynamic_slice_in_dim(normed, tp_index * own_count, own_count, 0).astype(
        jnp.float32
    )
    return layer_norm(ALPHA_RES * own_rows + expert_mix, gain_two, shift_two).astype(jnp.bfloat16)


GROUPS = 4


def fast_kernel(
    dims,
    qs_ref, ks_ref, vs_ref, ql_ref, kl_ref, vl_ref, bias_ref, stream_ref, os_ref, ol_ref,
    g1_ref, b1_ref, g2_ref, b2_ref, pick_ref, route_ref, wg_ref, wu_ref, wd_ref,
    out_ref,
    pack_a, pack_v, rq, rk, rv, rb, aq, ak, ao, ra, wos, wol, strm, pb, rp, st, rst, normed,
    place, xs, wsend, wrecv, ag, wg, wu, wd, hid, own_y, cs, cr, ts, rr, zs, zr, fs, fr,
    load_sem, q_send, q_recv, a_send, a_recv, p_send, p_recv, s_send, s_recv,
    x_send, x_recv, w_send, w_recv, g_send, g_recv, h_send, h_recv, c_send, c_recv,
    t_send, t_recv, z_send, z_recv, f_send, f_recv,
):
    n_sp, n_tp, rows, cols, cap, small_heads, hs, hl = dims
    f32, bf16 = jnp.float32, jnp.bfloat16
    sp = lax.axis_index("sp")
    tp = lax.axis_index("tp")
    core = lax.rem(sp, 2)
    chip = lax.div(sp, 2)
    sibling = sp + 1 - 2 * core
    n_z = n_sp // 2
    is_small = sp < small_heads
    large_heads = n_sp - small_heads
    ffw = wg_ref.shape[2]
    width = n_tp * cols

    def mesh_copy(src, dst, send, recv, target):
        return pltpu.make_async_remote_copy(
            src_ref=src, dst_ref=dst, send_sem=send, recv_sem=recv,
            device_id=target, device_id_type=pl.DeviceIdType.MESH,
        )

    def sp_at(j):
        return (j, tp)

    def tp_at(j):
        return (sp, j)

    def flip(index, mask, count):
        total, bit = 0, 1
        while bit < count:
            digit = lax.rem(lax.div(index, bit), 2)
            total = total + bit * (1 - digit if mask & bit else digit)
            bit *= 2
        return total

    z_masks = [0, n_z - 1, *range(1, n_z - 1)]
    z_order = [flip(chip, m, n_z) for m in z_masks]
    peers = [flip(tp, m, n_tp) for m in range(n_tp)]
    out_peers = [*peers[:0:-1], peers[0]]

    barrier = pltpu.get_barrier_semaphore()
    for k in range(1, n_sp):
        pl.semaphore_signal(barrier, inc=1, device_id=sp_at(lax.rem(sp + k, n_sp)), device_id_type=pl.DeviceIdType.MESH)
    for k in range(1, n_tp):
        pl.semaphore_signal(barrier, inc=1, device_id=tp_at(lax.rem(tp + k, n_tp)), device_id_type=pl.DeviceIdType.MESH)

    own_cols = pl.ds(pl.multiple_of(tp * cols, cols), cols)
    loads = [
        pltpu.make_async_copy(os_ref, wos, load_sem.at[0]),
        pltpu.make_async_copy(ol_ref, wol, load_sem.at[1]),
        pltpu.make_async_copy(stream_ref.at[:, own_cols], strm, load_sem.at[2]),
        pltpu.make_async_copy(wg_ref.at[0], wg, load_sem.at[3]),
        pltpu.make_async_copy(wu_ref.at[0], wu, load_sem.at[4]),
        pltpu.make_async_copy(wd_ref.at[0], wd, load_sem.at[5]),
    ]
    for load in loads:
        load.start()

    for h in range(small_heads):
        part = slice(h * hs, (h + 1) * hs)
        pack_a[h] = jnp.concatenate([qs_ref[:, part], ks_ref[:, part]], axis=1)
        pack_v[h] = jnp.concatenate([vs_ref[:rows // 2, part], vs_ref[rows // 2:, part]], axis=1)

    pl.semaphore_wait(barrier, n_sp + n_tp - 2)

    half_block = pl.ds(0, rows // 2)

    def head_copies(j, slot):
        if j < small_heads:
            pairs = [(0, pack_a.at[j], rq.at[slot]), (2, pack_v.at[j], rv.at[slot, half_block])]
        else:
            part = pl.ds((j - small_heads) * hl, hl)
            pairs = [
                (0, ql_ref.at[:, part], rq.at[slot]),
                (1, kl_ref.at[:, part], rk.at[slot]),
                (2, vl_ref.at[:, part], rv.at[slot]),
            ]
        pairs.append((3, bias_ref.at[j], rb.at[slot]))
        return pairs

    for distance in range(n_z):
        for j in range(n_sp):
            hops = jnp.maximum(j // 2 - chip, chip - j // 2)

            @pl.when((hops == distance) & (j != sp))
            def _():
                for kind, src, dst in head_copies(j, sp):
                    mesh_copy(src, dst, q_send.at[kind, j], q_recv.at[kind, sp], sp_at(j)).start()

    for j in range(n_sp):
        @pl.when(j == sp)
        def _():
            for kind, src, dst in head_copies(j, j):
                pltpu.make_async_copy(src, dst, q_recv.at[kind, j]).start()

    group = lax.div(pick_ref[0:1, :], 2)
    first_even = lax.rem(pick_ref[0:1, :], 2) == 0
    sub8 = lax.broadcasted_iota(jnp.int32, (8, rows), 0)
    one_hot = (sub8 == group).astype(f32)
    sub_r = lax.broadcasted_iota(jnp.int32, (rows, rows), 0)
    lane_r = lax.broadcasted_iota(jnp.int32, (rows, rows), 1)
    before = (sub_r < lane_r).astype(f32).astype(bf16)
    counts = jnp.dot(one_hot.astype(bf16), before, preferred_element_type=f32)
    rank = jnp.sum(one_hot * counts, axis=0, keepdims=True).astype(jnp.int32)
    slot_row = group * cap + rank
    slot_iota = lax.broadcasted_iota(jnp.int32, (GROUPS * cap, rows), 0)
    place[...] = (slot_iota == slot_row).astype(f32).astype(bf16)
    w_even = jnp.where(first_even, route_ref[0:1, :], route_ref[1:2, :])
    w_odd = jnp.where(first_even, route_ref[1:2, :], route_ref[0:1, :])
    w8 = jnp.where(sub8 == 0, w_even, jnp.where(sub8 == 1, w_odd, 0.0))
    w_hi = w8.astype(bf16)
    w_lo = (w8 - w_hi.astype(f32)).astype(bf16)
    for g in range(GROUPS):
        pick_g = ((sub_r == slot_row - g * cap) & (sub_r < cap)).astype(f32).astype(bf16)
        last = (((1,), (1,)), ((), ()))
        wsend[g] = lax.dot_general(w_hi, pick_g, last, preferred_element_type=f32) + lax.dot_general(
            w_lo, pick_g, last, preferred_element_type=f32
        )

    for j in range(n_sp):
        for kind in (0, 3):
            dst = (rq, None, None, rb)[kind].at[j]
            pltpu.make_async_copy(dst, dst, q_recv.at[kind, j]).wait()

    def unfold(packed):
        tall = jnp.concatenate([packed[:, :hs], packed[:, hs:]], axis=0)
        return jnp.concatenate([tall, jnp.zeros_like(tall)], axis=1)

    @pl.when(jnp.logical_not(is_small))
    def _():
        for j in range(n_sp):
            pltpu.make_async_copy(rk.at[j], rk.at[j], q_recv.at[1, j]).wait()
            pltpu.make_async_copy(rv.at[j], rv.at[j], q_recv.at[2, j]).wait()
            aq[pl.ds(j * rows, rows), :] = rq[j]
            ak[pl.ds(j * rows, rows), :] = rk[j]

    @pl.when(is_small)
    def _():
        lane = lax.broadcasted_iota(jnp.int32, (rows, hl), 1)
        for j in range(n_sp):
            folded = rv.at[j, half_block]
            pltpu.make_async_copy(folded, folded, q_recv.at[2, j]).wait()
            rv[j] = unfold(folded[...])
            both = rq[j]
            aq[pl.ds(j * rows, rows), :] = jnp.where(lane < hs, both, jnp.zeros_like(both))
            ak[pl.ds(j * rows, rows), :] = jnp.concatenate([both[:, hs:], both[:, :hs]], axis=1)

    for j in range(n_sp):
        @pl.when(j != sp)
        def _():
            for kind, src, dst in head_copies(j, sp):
                mesh_copy(src, dst, q_send.at[kind, j], q_recv.at[kind, sp], sp_at(j)).wait_send()

    scale = jnp.where(is_small, hs**-0.5, hl**-0.5).astype(f32)
    span = 2 * rows
    sub_t = lax.broadcasted_iota(jnp.int32, (span, span), 0)
    lane_t = lax.broadcasted_iota(jnp.int32, (span, span), 1)
    tri = (sub_t >= lane_t).astype(f32).astype(bf16)
    causal = lane_t < sub_t

    def tile(query, kj, diagonal, total, later):
        keys = ak[pl.ds(pl.multiple_of(kj * span, span), span), :]
        log_odds = jnp.concatenate([rb[2 * kj, 0:1, :], rb[2 * kj + 1, 0:1, :]], axis=1)
        score = lax.dot_general(query, keys, (((1,), (1,)), ((), ())), preferred_element_type=f32)
        score = score * scale + log_odds
        soft = jnp.maximum(score, 0.0) + jnp.log(1.0 + jnp.exp(-jnp.abs(score)))
        if diagonal:
            soft = jnp.where(causal, soft, 0.0)
        high = soft.astype(bf16)
        low = (soft - high.astype(f32)).astype(bf16)
        run = jnp.dot(high, tri, preferred_element_type=f32) + jnp.dot(low, tri, preferred_element_type=f32)
        stick = jnp.exp(score - run - later)
        if diagonal:
            stick = jnp.where(causal, stick, 0.0)
        values = jnp.concatenate([rv[2 * kj], rv[2 * kj + 1]], axis=0)
        total = total + jnp.dot(stick.astype(bf16), values, preferred_element_type=f32)
        return total, later + run[:, 0:1]

    def head_back(d, small):
        src, dst = (ao.at[d, half_block], ra.at[sp, half_block]) if small else (ao.at[d], ra.at[sp])
        return mesh_copy(src, dst, a_send.at[d], a_recv.at[sp], sp_at(d))

    for qi in range(n_sp // 2):
        query = aq[qi * span:(qi + 1) * span, :]
        carry = tile(query, qi, True, jnp.zeros((span, hl), f32), jnp.zeros((span, 1), f32))
        if qi:
            def visit(turn, carry):
                return tile(query, qi - 1 - turn, False, *carry)
            carry = lax.fori_loop(0, qi, visit, carry)
        for half in range(2):
            d = 2 * qi + half
            block = carry[0][half * rows:(half + 1) * rows].astype(bf16)

            @pl.when(is_small)
            def _():
                ao[d, :rows // 2, :] = jnp.concatenate([block[:rows // 2, :hs], block[rows // 2:, :hs]], axis=1)

            @pl.when(jnp.logical_not(is_small))
            def _():
                ao[d] = block
        for half in range(2):
            d = 2 * qi + half
            for small in (True, False):
                @pl.when((d != sp) & (is_small if small else jnp.logical_not(is_small)))
                def _():
                    head_back(d, small).start()

            if d < small_heads:
                own = pltpu.make_async_copy(ao.at[d, half_block], ra.at[d, half_block], a_recv.at[d])
            else:
                own = pltpu.make_async_copy(ao.at[d], ra.at[d], a_recv.at[d])

            @pl.when(d == sp)
            def _():
                own.start()

    for load in loads[:3]:
        load.wait()
    for j in range(n_sp):
        landed = ra.at[j, half_block] if j < small_heads else ra.at[j]
        pltpu.make_async_copy(landed, landed, a_recv.at[j]).wait()
    att_small = jnp.concatenate([unfold(ra[j, :rows // 2, :])[:, :hs] for j in range(small_heads)], axis=1)
    att_large = jnp.concatenate([ra[j] for j in range(small_heads, n_sp)], axis=1)

    def tp_wait_recv(buf, sem, src):
        pltpu.make_async_copy(buf.at[src], buf.at[src], sem.at[src]).wait()

    for k in range(1, n_tp + 1):
        t = out_peers[k - 1]
        part = pl.ds(pl.multiple_of(t * cols, cols), cols)
        term = jnp.dot(att_small, wos[:, part], preferred_element_type=f32)
        term = term + jnp.dot(att_large, wol[:, part], preferred_element_type=f32)
        pb[k - 1] = term.astype(bf16)
        if k < n_tp:
            mesh_copy(pb.at[k - 1], rp.at[tp], p_send.at[k], p_recv.at[tp], tp_at(t)).start()
    mixed = ALPHA_RES * strm[...].astype(f32) + pb[n_tp - 1].astype(f32)
    for k in range(1, n_tp):
        src = lax.rem(tp + k, n_tp)
        tp_wait_recv(rp, p_recv, src)
        mixed = mixed + rp[src].astype(f32)

    eye = sub_r == lane_r

    def to_row(column):
        return jnp.sum(jnp.where(eye, column, 0.0), axis=0, keepdims=True)

    def to_column(row):
        return jnp.sum(jnp.where(eye, row, 0.0), axis=1, keepdims=True)

    own_mean = jnp.mean(mixed, axis=1, keepdims=True)
    centred = mixed - own_mean
    own_square = jnp.sum(centred * centred, axis=1, keepdims=True)
    mean_row, square_row = to_row(own_mean), to_row(own_square)
    st[...] = jnp.where(sub8 == 0, mean_row, square_row)
    for k in range(1, n_tp):
        t = lax.rem(tp + k, n_tp)
        mesh_copy(st, rst.at[tp], s_send.at[k], s_recv.at[tp], tp_at(t)).start()
    means, squares = [mean_row], [square_row]
    for k in range(1, n_tp):
        src = lax.rem(tp + k, n_tp)
        tp_wait_recv(rst, s_recv, src)
        means.append(rst[src, 0:1, :])
        squares.append(rst[src, 1:2, :])
    full_mean = sum(means) / n_tp
    spread = sum(squares) + cols * sum((m - full_mean) * (m - full_mean) for m in means)
    scale_row = lax.rsqrt(spread / width + NORM_EPS)
    norm_val = (mixed - to_column(full_mean)) * to_column(scale_row) * g1_ref[:, own_cols] + b1_ref[:, own_cols]
    normed[...] = norm_val.astype(bf16)

    for g in range(GROUPS):
        xs[g] = jnp.dot(place[g * cap:(g + 1) * cap, :], normed[...], preferred_element_type=f32).astype(bf16)
    for k in range(n_z):
        g = z_order[k]
        dst = ag.at[core, tp, chip]
        if k == 0:
            pltpu.make_async_copy(xs.at[g], dst, x_recv.at[chip]).start()
        else:
            mesh_copy(xs.at[g], dst, x_send.at[k], x_recv.at[chip], sp_at(2 * g + core)).start()
    for k in range(n_sp):
        j = lax.rem(sp + k, n_sp)
        if k == 0:
            pltpu.make_async_copy(wsend.at[chip], wrecv.at[sp], w_recv.at[sp]).start()
        else:
            mesh_copy(wsend.at[lax.div(j, 2)], wrecv.at[sp], w_send.at[k], w_recv.at[sp], sp_at(j)).start()

    for z in z_order:
        piece = ag.at[core, tp, z]
        pltpu.make_async_copy(piece, piece, x_recv.at[z]).wait()
        for m in range(1, n_tp):
            mesh_copy(piece, piece, g_send.at[m, z], g_recv.at[tp, z], tp_at(peers[m])).start()
        mesh_copy(piece, piece, h_send.at[tp, z], h_recv.at[tp, z], sp_at(sibling)).start()
    for j in range(n_sp):
        pltpu.make_async_copy(wrecv.at[j], wrecv.at[j], w_recv.at[j]).wait()
    for load in loads[3:]:
        load.wait()

    other = 1 - core
    lane_c = lax.broadcasted_iota(jnp.int32, (cap, rows), 1)
    sub_c = lax.broadcasted_iota(jnp.int32, (cap, rows), 0)
    step = min(256, ffw)
    half = (n_z // 2) * cap

    def slot_weights(c, z):
        row = wrecv[2 * z + c, pl.ds(core, 1), :]
        return jnp.sum(jnp.where(sub_c == lane_c, row, 0.0), axis=1, keepdims=True)

    for p in range(2):
        zs_p = z_order[p * (n_z // 2):(p + 1) * (n_z // 2)]
        for z in zs_p:
            for m in range(1, n_tp):
                piece = ag.at[core, peers[m], z]
                pltpu.make_async_copy(piece, piece, g_recv.at[peers[m], z]).wait()
                mesh_copy(piece, piece, h_send.at[peers[m], z], h_recv.at[peers[m], z], sp_at(sibling)).start()
        for z in zs_p:
            for t in range(n_tp):
                piece = ag.at[other, t, z]
                pltpu.make_async_copy(piece, piece, h_recv.at[t, z]).wait()
        weights = jnp.concatenate([slot_weights(c, z) for c in (other, core) for z in zs_p], axis=0)

        def body(n, carry):
            part = pl.ds(pl.multiple_of(n * step, step), step)
            gate = jnp.zeros((2 * half, step), f32)
            upper = jnp.zeros((2 * half, step), f32)
            for t in range(n_tp):
                x = jnp.concatenate([ag[c, t, z] for c in (other, core) for z in zs_p], axis=0)
                gate = gate + jnp.dot(x, wg[t * cols:(t + 1) * cols, part], preferred_element_type=f32)
                upper = upper + jnp.dot(x, wu[t * cols:(t + 1) * cols, part], preferred_element_type=f32)
            hid[:, part] = (gate / (1.0 + jnp.exp(-gate)) * upper).astype(bf16)
            return carry

        lax.fori_loop(0, ffw // step, body, 0)

        def join(k):
            pltpu.make_async_copy(cr.at[p, k], cr.at[p, k], c_recv.at[p, k]).wait()
            both = own_y[p, k] + cr[p, k].astype(f32)
            if k == n_tp - 1:
                own_y[p, k] = both
                return
            for i in range(n_z // 2):
                kz = p * (n_z // 2) + i
                ts[k, kz] = both[i * cap:(i + 1) * cap].astype(bf16)
                mesh_copy(
                    ts.at[k, kz], rr.at[tp, kz], t_send.at[k, kz], t_recv.at[tp, kz], tp_at(out_peers[k])
                ).start()

        for k in range(n_tp):
            part = pl.ds(pl.multiple_of(out_peers[k] * cols, cols), cols)
            y = jnp.dot(hid[...], wd[:, part], preferred_element_type=f32) * weights
            cs[p, k] = y[:half].astype(bf16)
            mesh_copy(cs.at[p, k], cr.at[p, k], c_send.at[p, k], c_recv.at[p, k], sp_at(sibling)).start()
            own_y[p, k] = y[half:]
            if k:
                join(k - 1)
        join(n_tp - 1)

    for kz in range(n_z):
        z = z_order[kz]
        i = kz % (n_z // 2)
        total = own_y[kz // (n_z // 2), n_tp - 1, i * cap:(i + 1) * cap, :]
        for m in range(1, n_tp):
            src = peers[m]
            pltpu.make_async_copy(rr.at[src, kz], rr.at[src, kz], t_recv.at[src, kz]).wait()
            total = total + rr[src, kz].astype(f32)
        zs[kz] = total.astype(bf16)
        if kz:
            mesh_copy(zs.at[kz], zr.at[chip], z_send.at[kz], z_recv.at[chip], sp_at(2 * z + core)).start()
        else:
            pltpu.make_async_copy(zs.at[kz], zr.at[chip], z_recv.at[chip]).start()
    for z in range(n_z):
        pltpu.make_async_copy(zr.at[z], zr.at[z], z_recv.at[z]).wait()
    expert_mix = lax.dot_general(
        place[...], zr[...].reshape(n_z * cap, cols), (((0,), (0,)), ((), ())), preferred_element_type=f32
    )
    final = ALPHA_RES * normed[...].astype(f32) + expert_mix
    own_rows = rows // n_tp
    for t in range(n_tp):
        fs[t] = final[t * own_rows:(t + 1) * own_rows]
    for k in range(1, n_tp):
        t = lax.rem(tp + k, n_tp)
        mesh_copy(fs.at[t], fr.at[tp], f_send.at[k], f_recv.at[tp], tp_at(t)).start()
    keep = pltpu.make_async_copy(fs.at[tp], fr.at[tp], f_recv.at[tp])
    keep.start()
    for t in range(n_tp):
        tp_wait_recv(fr, f_recv, t)
    blocks = [fr[t] for t in range(n_tp)]
    average = sum(jnp.sum(b, axis=1, keepdims=True) for b in blocks) / width
    blocks = [b - average for b in blocks]
    variance = sum(jnp.sum(b * b, axis=1, keepdims=True) for b in blocks) / width
    inverse = lax.rsqrt(variance + NORM_EPS)
    for t in range(n_tp):
        part = slice(t * cols, (t + 1) * cols)
        out_ref[:, part] = (blocks[t] * inverse * g2_ref[:, part] + b2_ref[:, part]).astype(bf16)

    for d in range(n_sp):
        for small in (True, False):
            @pl.when((d != sp) & (is_small if small else jnp.logical_not(is_small)))
            def _():
                head_back(d, small).wait_send()
    for k in range(1, n_sp):
        j = lax.rem(sp + k, n_sp)
        mesh_copy(wsend.at[lax.div(j, 2)], wrecv.at[sp], w_send.at[k], w_recv.at[sp], sp_at(j)).wait_send()
    for k in range(1, n_tp):
        t = lax.rem(tp + k, n_tp)
        mesh_copy(pb.at[k - 1], rp.at[tp], p_send.at[k], p_recv.at[tp], tp_at(out_peers[k - 1])).wait_send()
        mesh_copy(st, rst.at[tp], s_send.at[k], s_recv.at[tp], tp_at(t)).wait_send()
        mesh_copy(fs.at[t], fr.at[tp], f_send.at[k], f_recv.at[tp], tp_at(t)).wait_send()
        for z in range(n_z):
            piece = ag.at[core, tp, z]
            mesh_copy(piece, piece, g_send.at[k, z], g_recv.at[tp, z], tp_at(peers[k])).wait_send()
            mesh_copy(
                ts.at[k - 1, z], rr.at[tp, z], t_send.at[k - 1, z], t_recv.at[tp, z], tp_at(out_peers[k - 1])
            ).wait_send()
    for k in range(1, n_z):
        g = z_order[k]
        mesh_copy(xs.at[g], ag.at[core, tp, chip], x_send.at[k], x_recv.at[chip], sp_at(2 * g + core)).wait_send()
        mesh_copy(zs.at[k], zr.at[chip], z_send.at[k], z_recv.at[chip], sp_at(2 * g + core)).wait_send()
    for t in range(n_tp):
        for p in range(2):
            mesh_copy(cs.at[p, t], cr.at[p, t], c_send.at[p, t], c_recv.at[p, t], sp_at(sibling)).wait_send()
        for z in range(n_z):
            piece = ag.at[core, t, z]
            mesh_copy(piece, piece, h_send.at[t, z], h_recv.at[t, z], sp_at(sibling)).wait_send()


def fast_local(
    stream, query_small, key_small, value_small, query_large, key_large, value_large, key_bias,
    out_small, out_large, gain_one, shift_one, gain_two, shift_two, expert_pick, route_weight,
    w_gate, w_up, w_down,
):
    f32, bf16 = jnp.float32, jnp.bfloat16
    n_sp, n_tp = lax.axis_size("sp"), lax.axis_size("tp")
    rows, width = stream.shape
    cols = width // n_tp
    hs, hl = HEAD_SMALL, HEAD_LARGE
    small_heads = query_small.shape[1] // hs
    cap = 4 * rows // (w_gate.shape[0] * n_sp)
    n_z = n_sp // 2
    ffw = w_gate.shape[2]
    bias = key_bias.astype(f32).transpose(1, 2, 0).reshape(n_sp, 1, rows)
    bias = jnp.broadcast_to(bias, (n_sp, 8, rows))
    vmem = pl.BlockSpec(memory_space=pltpu.VMEM)
    hbm = pl.BlockSpec(memory_space=pl.ANY)
    dma = pltpu.SemaphoreType.DMA
    V = pltpu.VMEM
    half = n_z * cap
    scratch = [
        V((small_heads, rows, hl), bf16), V((small_heads, rows // 2, hl), bf16),
        V((n_sp, rows, hl), bf16), V((n_sp, rows, hl), bf16), V((n_sp, rows, hl), bf16),
        V((n_sp, 8, rows), f32),
        V((n_sp * rows, hl), bf16), V((n_sp * rows, hl), bf16),
        V((n_sp, rows, hl), bf16), V((n_sp, rows, hl), bf16),
        V(out_small.shape, bf16), V(out_large.shape, bf16), V((rows, cols), bf16),
        V((n_tp, rows, cols), bf16), V((n_tp, rows, cols), bf16),
        V((8, rows), f32), V((n_tp, 8, rows), f32), V((rows, cols), bf16),
        V((GROUPS * cap, rows), bf16), V((GROUPS, cap, cols), bf16),
        V((GROUPS, 8, rows), f32), V((n_sp, 8, rows), f32),
        V((2, n_tp, n_z, cap, cols), bf16),
        V((width, ffw), bf16), V((width, ffw), bf16), V((ffw, width), bf16),
        V((half, ffw), bf16), V((2, n_tp, half // 2, cols), f32),
        V((2, n_tp, half // 2, cols), bf16), V((2, n_tp, half // 2, cols), bf16),
        V((n_tp - 1, n_z, cap, cols), bf16), V((n_tp, n_z, cap, cols), bf16),
        V((n_z, cap, cols), bf16), V((n_z, cap, cols), bf16),
        V((n_tp, rows // n_tp, cols), f32), V((n_tp, rows // n_tp, cols), f32),
        dma((6,)), dma((4, n_sp)), dma((4, n_sp)), dma((n_sp,)), dma((n_sp,)),
        dma((n_tp,)), dma((n_tp,)), dma((n_tp,)), dma((n_tp,)),
        dma((n_z,)), dma((n_z,)), dma((n_sp,)), dma((n_sp,)),
        dma((n_tp, n_z)), dma((n_tp, n_z)), dma((n_tp, n_z)), dma((n_tp, n_z)),
        dma((2, n_tp)), dma((2, n_tp)), dma((n_tp, n_z)), dma((n_tp, n_z)),
        dma((n_z,)), dma((n_z,)), dma((n_tp,)), dma((n_tp,)),
    ]
    dims = (n_sp, n_tp, rows, cols, cap, small_heads, hs, hl)
    return pl.pallas_call(
        functools.partial(fast_kernel, dims),
        out_shape=jax.ShapeDtypeStruct((rows // n_tp, width), bf16),
        in_specs=[vmem] * 7 + [hbm] * 3 + [vmem] * 6 + [hbm] * 3,
        out_specs=vmem,
        scratch_shapes=scratch,
        compiler_params=pltpu.CompilerParams(
            collective_id=0, has_side_effects=True, vmem_limit_bytes=60 * 1024 * 1024
        ),
        name="layer",
    )(
        query_small, key_small, value_small, query_large, key_large, value_large, bias,
        stream, out_small, out_large,
        gain_one[None], shift_one[None], gain_two[None], shift_two[None],
        expert_pick.T, route_weight.T, w_gate, w_up, w_down,
    )


def layer(*arrays):
    n_sp, n_tp = lax.axis_size("sp"), lax.axis_size("tp")
    heads = arrays[1].shape[1] // HEAD_SMALL + arrays[4].shape[1] // HEAD_LARGE
    experts = arrays[16].shape[0] * n_sp
    paired = experts == 2 * GROUPS and n_sp == experts
    if paired and heads == n_sp and arrays[7].shape[2] * 2 == n_sp and arrays[0].shape[1] % (128 * n_tp) == 0:
        return fast_local(*arrays)
    return local(*arrays)


def solution(mesh):
    placed = (
        P("sp", None),
        P("sp", "tp"),
        P("sp", "tp"),
        P("sp", "tp"),
        P("sp", "tp"),
        P("sp", "tp"),
        P("sp", "tp"),
        P("sp", None, "tp"),
        P("tp", None),
        P("tp", None),
        P(),
        P(),
        P(),
        P(),
        P("sp", None),
        P("sp", None),
        P("sp", None, "tp"),
        P("sp", None, "tp"),
        P("sp", "tp", None),
    )
    return jax.shard_map(
        layer, mesh=mesh, in_specs=placed, out_specs=P(("sp", "tp"), None), check_vma=False
    )
```
